512 devices in a mesh: sp: 64 (over z, y), tp: 8 (over x, core).
Axes of the slice: x: 4, y: 8, z: 8, core: 2. Of those that a mesh axis runs over, the one named last changes fastest.
Arguments:
- tokens: bfloat16 [20480, 2048], P('sp', 'tp'), may hold values from -6 to 6
- norm_gain: float32 [2048], replicated, may hold values from 0.1 to 1.9
- w_qa: bfloat16 [2048, 1024], P(None, 'tp'), may hold values from -1 to 1
- w_ka: bfloat16 [2048, 512], P(None, 'tp'), may hold values from -1 to 1
- w_va: bfloat16 [2048, 512], P(None, 'tp'), may hold values from -0.125 to 0.125
- qgain_a: float32 [16, 64], P('tp'), may hold values from 0.2 to 9
- kgain_a: float32 [8, 64], P('tp'), may hold values from 0.2 to 9
- w_qb: bfloat16 [2048, 1024], P(None, 'tp'), may hold values from -10 to 10
- w_kb: bfloat16 [2048, 512], P(None, 'tp'), may hold values from -1 to 1
- w_vb: bfloat16 [2048, 512], P(None, 'tp'), may hold values from -0.125 to 0.125
- sink_b: float32 [16], P('tp'), may hold values from 3 to 8
- w_ga: bfloat16 [2048, 1024], P(None, 'tp'), may hold values from -0.125 to 0.125
- w_gb: bfloat16 [2048, 1024], P(None, 'tp'), may hold values from -0.125 to 0.125
- out_a: bfloat16 [1024, 2048], P('tp'), may hold values from -0.375 to 0.375
- out_b: bfloat16 [1024, 2048], P('tp'), may hold values from -0.375 to 0.375
Outputs:
- mixed: bfloat16 [20480, 2048], P(('sp', 'tp'))
The draws below stay inside these ranges and needn't reach their ends.
All inputs are finite; a program needn't handle non-finite values.
Results may differ from the reference program's by a relative error of at most 0.028.
Values may be sent and summed in bfloat16 or wider, within the bound.
No kernel may reach another device: no remote copies, remote signals or barrier semaphores. Data moves between devices by JAX's collectives and lax.ppermute only.
A program may use at most 64 MiB of HBM per device.

```python
import math
import jax
import jax.numpy as jnp
from jax import lax

D = 2048
HEAD = 64
HA = 16
KA = 8
HB = 16
KB = 8
GRID = 64
WINDOW = 128
SEQ = 20480
N_TP = 8


def rough_matrix(key, height, breadth, spread):
    return jnp.clip(jax.random.normal(key, (height, breadth), jnp.float32), -6.0, 6.0) * spread


def head_gains(key, heads):
    levels = jnp.exp(jax.random.uniform(jax.random.fold_in(key, 1), (heads, 1), jnp.float32, -0.2231, 0.9163))
    jitter = 1.0 + 0.18 * jnp.clip(jax.random.normal(jax.random.fold_in(key, 2), (heads, HEAD), jnp.float32), -2.5, 2.5)
    return levels * jitter


def key_matrix_a(key):
    return rough_matrix(jax.random.fold_in(key, 41), D, KA * HEAD, D ** (-0.5))


def key_matrix_b(key):
    return rough_matrix(jax.random.fold_in(key, 51), D, KB * HEAD, D ** (-0.5))


def draw_qgain_a(key, part):
    return head_gains(jax.random.fold_in(key, 31), HA)


def draw_kgain_a(key, part):
    return head_gains(jax.random.fold_in(key, 32), KA)


def draw_w_ka(key, part):
    return key_matrix_a(key).astype(jnp.bfloat16)


def draw_w_qa(key, part):
    base = rough_matrix(jax.random.fold_in(key, 42), D, HA * HEAD, D ** (-0.5))
    return base.astype(jnp.bfloat16)


def draw_w_kb(key, part):
    return key_matrix_b(key).astype(jnp.bfloat16)


def draw_w_qb(key, part):
    base = rough_matrix(jax.random.fold_in(key, 52), D, HB * HEAD, 2.0 * D ** (-0.5))
    return base.astype(jnp.bfloat16)


def block_scale(stream_key, dims, pieces, smallest, high):
    factor_of = 1.0
    for dim, blocks in pieces:
        heights = jax.random.uniform(jax.random.fold_in(jax.random.fold_in(stream_key, 6), dim), (blocks,), jnp.float32, smallest / len(pieces), high / len(pieces))
        factor_of = factor_of * jnp.repeat(jnp.exp(heights), dims[dim] // blocks).reshape((-1,) + (1,) * (len(dims) - 1 - dim))
    return factor_of


def scatter_about(stream_key, dims, scale, limit, pieces=(), kind=jnp.bfloat16):
    drawn = scale * jax.random.normal(stream_key, dims, jnp.float32)
    if pieces:
        drawn = drawn * block_scale(stream_key, dims, pieces, -0.22, 0.18)
    return jnp.clip(drawn, -limit, limit).astype(kind)


def setup_inputs(seed: int = 0) -> dict:
    splits = jax.random.split(jax.random.key(seed), 16)
    return {
        "tokens": scatter_about(splits[0], (SEQ, D), 1.0, 6.0, ((0, 64), (1, 8))),
        "norm_gain": jnp.clip(1.0 + 0.18 * jax.random.normal(splits[1], (D,), jnp.float32), 0.1, 1.9),
        "w_qa": draw_w_qa(jax.random.fold_in(splits[15], 71), 0),
        "w_ka": draw_w_ka(jax.random.fold_in(splits[15], 71), 0),
        "w_va": scatter_about(splits[4], (D, KA * HEAD), D ** -0.5, 0.125, ((1, 8),)),
        "qgain_a": draw_qgain_a(jax.random.fold_in(splits[15], 71), 0),
        "kgain_a": draw_kgain_a(jax.random.fold_in(splits[15], 71), 0),
        "w_qb": draw_w_qb(jax.random.fold_in(splits[15], 71), 0),
        "w_kb": draw_w_kb(jax.random.fold_in(splits[15], 71), 0),
        "w_vb": scatter_about(splits[9], (D, KB * HEAD), D ** -0.5, 0.125, ((1, 8),)),
        "sink_b": jnp.clip(3.0 + 5.0 * jax.random.uniform(splits[10], (HB,), jnp.float32) ** block_scale(splits[10], (HB,), ((0, 8),), -0.2, 0.2), 3.0, 8.0),
        "w_ga": scatter_about(splits[11], (D, HA * HEAD), D ** -0.5, 0.125, ((1, 8),)),
        "w_gb": scatter_about(splits[12], (D, HB * HEAD), D ** -0.5, 0.125, ((1, 8),)),
        "out_a": scatter_about(splits[13], (HA * HEAD, D), (HA * HEAD // 4) ** -0.5, 0.375, ((0, 8),)),
        "out_b": scatter_about(splits[14], (HB * HEAD, D), (HB * HEAD // 4) ** -0.5, 0.375, ((0, 8),)),
    }


EPSILON = 1e-06
THETA = 10000.0

def head_norm(values, head_gain):
    return values * lax.rsqrt(lax.optimization_barrier(jnp.mean(values * values, axis=-1, keepdims=True)) + EPSILON) * head_gain

def turn_half(values, angles):
    first, second = jnp.split(values, 2, axis=-1)
    cosine = jnp.cos(angles)[:, None, :]
    sine_part = jnp.sin(angles)[:, None, :]
    return jnp.concatenate([first * cosine - second * sine_part, first * sine_part + second * cosine], axis=-1)

def grid_rotary(values, position):
    half_width = values.shape[-1] // 2
    quarter = half_width // 2
    frequency = jnp.power(THETA, -jnp.arange(quarter, dtype=jnp.float32) / quarter)
    row_angle = (position // GRID).astype(jnp.float32)[:, None] * frequency
    column_angle = (position % GRID).astype(jnp.float32)[:, None] * frequency
    return jnp.concatenate([turn_half(values[..., :half_width], row_angle), turn_half(values[..., half_width:], column_angle)], axis=-1)

def global_attention(queries, key_rows, values):
    length = queries.shape[0]
    group_size = HA // KA
    block_size = math.gcd(length, 128)
    key_float = key_rows.astype(jnp.float32)
    value_float = values.astype(jnp.float32)
    query_blocks = queries.astype(jnp.float32).reshape(length // block_size, block_size, KA, group_size, HEAD)

    def one_block(query_block):
        scores = jnp.einsum('qkgd,skd->kgqs', query_block, key_float) * HEAD ** (-0.5)
        row_max = lax.optimization_barrier(jnp.max(scores, axis=-1, keepdims=True))
        exponent_terms = jnp.exp(scores - row_max)
        denominator = lax.optimization_barrier(jnp.sum(exponent_terms, axis=-1))
        weights_low = lax.optimization_barrier(exponent_terms.astype(jnp.bfloat16)).astype(jnp.float32)
        mixed_block = jnp.einsum('kgqs,skd->qkgd', weights_low, value_float)
        return mixed_block / jnp.transpose(denominator, (2, 0, 1))[..., None]
    return lax.map(one_block, query_blocks).reshape(length, HA * HEAD)

def window_attention(queries, key_rows, values, sink_logit):
    length = queries.shape[0]
    group_size = HB // KB
    block_size = math.gcd(length, 128)
    span_size = block_size + 2 * WINDOW
    padded_keys = jnp.pad(key_rows.astype(jnp.float32), ((WINDOW, WINDOW), (0, 0), (0, 0)))
    padded_values = jnp.pad(values.astype(jnp.float32), ((WINDOW, WINDOW), (0, 0), (0, 0)))
    query_blocks = queries.astype(jnp.float32).reshape(length // block_size, block_size, KB, group_size, HEAD)
    offsets = jnp.arange(span_size, dtype=jnp.int32) - WINDOW
    relative = offsets[None, :] - jnp.arange(block_size, dtype=jnp.int32)[:, None]
    sink_heads = sink_logit.reshape(KB, group_size)[:, :, None]

    def one_block(inputs):
        block_index, query_block = inputs
        first_row = (block_index * block_size).astype(jnp.int32)
        keys_here = lax.dynamic_slice_in_dim(padded_keys, first_row, span_size, 0)
        values_here = lax.dynamic_slice_in_dim(padded_values, first_row, span_size, 0)
        absolute = first_row + offsets
        allowed = (jnp.abs(relative) <= WINDOW) & (absolute >= 0)[None, :] & (absolute < length)[None, :]
        scores = jnp.einsum('qkgd,skd->kgqs', query_block, keys_here) * HEAD ** (-0.5)
        scores = jnp.where(allowed, scores, -jnp.inf)
        row_max = jnp.maximum(lax.optimization_barrier(jnp.max(scores, axis=-1)), sink_heads)
        exponent_terms = jnp.exp(scores - row_max[..., None])
        denominator = lax.optimization_barrier(jnp.sum(exponent_terms, axis=-1)) + jnp.exp(sink_heads - row_max)
        weights_low = lax.optimization_barrier(exponent_terms.astype(jnp.bfloat16)).astype(jnp.float32)
        mixed_block = jnp.einsum('kgqs,skd->qkgd', weights_low, values_here)
        return mixed_block / jnp.transpose(denominator, (2, 0, 1))[..., None]
    indices = jnp.arange(length // block_size, dtype=jnp.int32)
    return lax.map(one_block, (indices, query_blocks)).reshape(length, HB * HEAD)

def reference(tokens, norm_gain, w_qa, w_ka, w_va, qgain_a, kgain_a, w_qb, w_kb, w_vb, sink_b, w_ga, w_gb, out_a, out_b):
    length = tokens.shape[0]
    features = tokens.astype(jnp.float32)
    normed = (features * lax.rsqrt(lax.optimization_barrier(jnp.mean(features * features, axis=-1, keepdims=True)) + EPSILON) * norm_gain).astype(jnp.bfloat16)

    def project(weight):
        return jnp.dot(normed, weight, preferred_element_type=jnp.float32).astype(jnp.bfloat16)
    position = jnp.arange(length, dtype=jnp.int32)
    query_a = grid_rotary(head_norm(project(w_qa).astype(jnp.float32).reshape(length, HA, HEAD), qgain_a), position).astype(jnp.bfloat16)
    key_a = grid_rotary(head_norm(project(w_ka).astype(jnp.float32).reshape(length, KA, HEAD), kgain_a), position).astype(jnp.bfloat16)
    value_a = project(w_va).reshape(length, KA, HEAD)
    attend_a = global_attention(query_a, key_a, value_a)
    attend_b = window_attention(project(w_qb).reshape(length, HB, HEAD), project(w_kb).reshape(length, KB, HEAD), project(w_vb).reshape(length, KB, HEAD), sink_b)
    gated_a = (attend_a * jax.nn.silu(project(w_ga).astype(jnp.float32))).astype(jnp.bfloat16)
    gated_b = (attend_b * jax.nn.silu(project(w_gb).astype(jnp.float32))).astype(jnp.bfloat16)
    width_a = HA * HEAD // N_TP
    width_b = HB * HEAD // N_TP
    summed = jnp.zeros((length, D), jnp.float32)
    for block_index in range(N_TP):
        lower_a = block_index * width_a
        lower_b = block_index * width_b
        partial_term = jnp.dot(gated_a[:, lower_a:lower_a + width_a], out_a[lower_a:lower_a + width_a], preferred_element_type=jnp.float32)
        partial_term = partial_term + jnp.dot(gated_b[:, lower_b:lower_b + width_b], out_b[lower_b:lower_b + width_b], preferred_element_type=jnp.float32)
        summed = summed + lax.optimization_barrier(partial_term.astype(jnp.bfloat16)).astype(jnp.float32)
    return summed.astype(jnp.bfloat16)
```

```python
import functools

import jax
import jax.numpy as jnp
import numpy as np
from jax import lax
from jax.experimental import pallas as pl
from jax.experimental.pallas import tpu as pltpu
from jax.sharding import Mesh, PartitionSpec as P

GRID = 64
WINDOW = 128
EPSILON = 1e-06
THETA = 10000.0
HEAD = 64
LANES = 128
BOUND = 69.0
SHIFT = 55.0
STAT_ROWS = 24
ACC_ROWS = 80
F32 = jnp.float32
BF16 = jnp.bfloat16


def whole(shape, space=pltpu.VMEM):
    return pl.BlockSpec(memory_space=space)


def rotary_tables(seq):
    quarter = HEAD // 4
    freq = np.power(np.float32(THETA), -np.arange(quarter, dtype=np.float32) / np.float32(quarter))
    freq = freq.astype(np.float32)

    def table(count, which):
        angle = (np.arange(count, dtype=np.float32)[:, None] * freq).astype(np.float64)
        out = []
        for fn in (np.cos, np.sin):
            half = np.concatenate([fn(angle), fn(angle)], axis=1)
            zero = np.zeros_like(half)
            head = np.concatenate([half, zero] if which == 0 else [zero, half], axis=1)
            out.append(np.concatenate([head, head], axis=1).astype(np.float32))
        return np.stack(out)

    return table(seq // GRID, 0), table(GRID, 1)


def dot(a, b):
    return jnp.dot(a, b, preferred_element_type=F32)


def dot_t(a, b):
    return lax.dot_general(a, b, (((1,), (1,)), ((), ())), preferred_element_type=F32)


def silu(v):
    return v / (1.0 + jnp.exp(-v))


def project_kernel(
    core_ref, mine_ref, other_ref, gain_ref, wqa, wka, wva, wqb, wkb, wvb, wga, wgb,
    qgain_ref, kgain_ref, row_ref, col_ref,
    q_out, kv_out, qb_out, kvb_out, ga_out, gb_out, h_s,
):
    core = core_ref[0]
    chips, rows, width = mine_ref.shape
    total = jnp.zeros((rows, 1), F32)
    for ref in (mine_ref, other_ref):
        for i in range(chips):
            part = ref[i].astype(F32)
            total = total + jnp.sum(part * part, axis=1, keepdims=True)
    scale = lax.rsqrt(total / (2 * chips * width) + EPSILON)
    for ref, side in ((mine_ref, core), (other_ref, 1 - core)):
        for i in range(chips):
            t = 2 * i + side
            h_s[t] = (ref[i].astype(F32) * scale * gain_ref[t]).astype(BF16)
    normed = jnp.concatenate([h_s[t] for t in range(2 * chips)], axis=1)
    both_q = dot(normed, jnp.concatenate([wqa[...], wqb[...]], axis=1))
    both_kv = dot(normed, jnp.concatenate([wka[...], wva[...], wkb[...], wvb[...]], axis=1))
    both_g = dot(normed, jnp.concatenate([wga[...], wgb[...]], axis=1))
    ga_out[...] = both_g[:, :LANES].astype(BF16)
    gb_out[...] = both_g[:, LANES:].astype(BF16)
    qb_out[...] = both_q[:, LANES:].astype(BF16)
    kvb_out[...] = both_kv[:, LANES:].astype(BF16)
    cos = []
    sin = []
    for r in range(rows // GRID):
        cos.append(row_ref[0, r : r + 1, :] + col_ref[0])
        sin.append(row_ref[1, r : r + 1, :] + col_ref[1])
    cos = jnp.concatenate(cos, axis=0)
    sin = jnp.concatenate(sin, axis=0)
    lane = lax.broadcasted_iota(jnp.int32, (rows, LANES), 1)
    first = (lane % 32) < 16
    low = lane < HEAD

    def turned(v, gain):
        return_v = v * v
        sum_low = jnp.sum(jnp.where(low, return_v, 0.0), axis=1, keepdims=True)
        sum_all = jnp.sum(return_v, axis=1, keepdims=True)
        rs_low = lax.rsqrt(sum_low / HEAD + EPSILON)
        rs_high = lax.rsqrt((sum_all - sum_low) / HEAD + EPSILON)
        n = v * jnp.where(low, rs_low, rs_high) * gain
        partner = jnp.where(first, -pltpu.roll(n, LANES - 16, 1), pltpu.roll(n, 16, 1))
        return n * cos + partner * sin

    qa = turned(both_q[:, :LANES].astype(BF16).astype(F32), qgain_ref[...]).astype(BF16)
    for i in range(q_out.shape[0]):
        q_out[i] = qa
    kv = both_kv[:, :LANES].astype(BF16).astype(F32)
    k_only = jnp.where(low, kv, 0.0)
    sq = jnp.sum(k_only * k_only, axis=1, keepdims=True)
    n = k_only * lax.rsqrt(sq / HEAD + EPSILON) * kgain_ref[...]
    partner = jnp.where(first, -pltpu.roll(n, LANES - 16, 1), pltpu.roll(n, 16, 1))
    ka = n * cos + partner * sin
    kv_out[...] = jnp.where(low, ka, kv).astype(BF16)


def window_kernel(index_ref, q_ref, mid_ref, prev_ref, next_ref, sink_ref, gate_ref, out_ref):
    s_index = index_ref[0]
    count = index_ref[1]
    rows = q_ref.shape[0]
    kv = jnp.concatenate([prev_ref[...], mid_ref[...], next_ref[...]], axis=0)
    span = kv.shape[0]
    r = lax.broadcasted_iota(jnp.int32, (rows, span), 0)
    c = lax.broadcasted_iota(jnp.int32, (rows, span), 1)
    place = s_index * rows - WINDOW + c
    allowed = (c >= r) & (c - r <= 2 * WINDOW) & (place >= 0) & (place < rows * count)
    keys = kv[:, :HEAD]
    values = kv[:, HEAD:]
    outs = []
    for h in range(2):
        s = dot_t(q_ref[:, h * HEAD : (h + 1) * HEAD], keys) * HEAD ** (-0.5)
        s = jnp.where(allowed, s, -1e30)
        sink = sink_ref[h]
        top = jnp.maximum(jnp.max(s, axis=1, keepdims=True), sink)
        p = jnp.where(allowed, jnp.exp(s - top), 0.0)
        den = jnp.sum(p, axis=1, keepdims=True) + jnp.exp(sink - top)
        outs.append(dot(p.astype(BF16), values) / den)
    att = jnp.concatenate(outs, axis=1)
    out_ref[...] = (att * silu(gate_ref[...].astype(F32))).astype(BF16)


def attend_kernel(q_ref, kv_ref, out_ref, k_s, vt_s, qt_s, m_s, o_s, lse_s, *, tile, chunk):
    n_q = q_ref.shape[0]
    n_k = kv_ref.shape[0]
    tiles = n_q // tile
    chunks = n_k // chunk
    kv = kv_ref[...]
    lane = lax.broadcasted_iota(jnp.int32, (n_k, LANES), 1)
    ones = jnp.where(lane < HEAD + 3, 1.0, 0.0)
    k_s[...] = jnp.where(lane < HEAD, kv.astype(F32), ones).astype(BF16)
    kv_t = kv.astype(F32).T
    k_t = kv_t[:HEAD]
    k_norm = jnp.max(jnp.sum(k_t * k_t, axis=0, keepdims=True))
    vt_s[:HEAD] = kv_t[HEAD:].astype(BF16)
    row16 = lax.broadcasted_iota(jnp.int32, (ACC_ROWS - HEAD, n_k), 0)
    vt_s[HEAD:] = jnp.where(row16 == 0, 1.0, 0.0).astype(BF16)
    top = jnp.float32(0.0)
    for i in range(tiles):
        q_t = q_ref[i * tile : (i + 1) * tile, :].astype(F32).T
        for h in range(2):
            part = q_t[h * HEAD : (h + 1) * HEAD] * HEAD ** (-0.5)
            bound = jnp.sqrt(jnp.sum(part * part, axis=0, keepdims=True) * k_norm) * 1.0001
            top = jnp.maximum(top, jnp.max(bound))
            m_s[2 * i + h] = bound - SHIFT
            qt_s[2 * i + h, :HEAD] = part.astype(BF16)
            qt_s[2 * i + h, HEAD:] = jnp.zeros((LANES - HEAD, tile), BF16)

    @pl.when(top > BOUND)
    def _():
        def row_max(t, carry):
            def one(c, m):
                s = dot(k_s[pl.ds(pl.multiple_of(c * chunk, chunk), chunk), :], qt_s[t])
                return jnp.maximum(m, jnp.max(s, axis=0, keepdims=True))

            m_s[t] = lax.fori_loop(0, chunks, one, jnp.full((1, tile), -1e30, F32))
            return carry

        lax.fori_loop(0, 2 * tiles, row_max, 0)

    row = lax.broadcasted_iota(jnp.int32, (16, tile), 0)

    def one_tile(i, carry):
        halves = []
        for h in range(2):
            t = 2 * i + h
            m = m_s[t]
            neg = -m
            hi = neg.astype(BF16).astype(F32)
            mid = (neg - hi).astype(BF16).astype(F32)
            lo = neg - hi - mid
            parts = jnp.where(row == 0, hi, jnp.where(row == 1, mid, jnp.where(row == 2, lo, 0.0)))
            qt_s[t, HEAD : HEAD + 16] = parts.astype(BF16)
            q_here = qt_s[t]
            acc = jnp.zeros((ACC_ROWS, tile), F32)
            for c in range(chunks):
                s = dot(k_s[c * chunk : (c + 1) * chunk, :], q_here)
                p = jnp.exp(s).astype(BF16)
                acc = acc + dot(vt_s[:, c * chunk : (c + 1) * chunk], p)
            total = acc[HEAD : HEAD + 1]
            halves.append(acc[:HEAD] / total)
            lse_s[t] = m + jnp.log(total)
        o_t = jnp.concatenate(halves, axis=0)
        o_s[pl.ds(pl.multiple_of(i * tile, tile), tile), :] = o_t.T.astype(BF16)
        return carry

    lax.fori_loop(0, tiles, one_tile, 0)

    lse = jnp.concatenate(
        [jnp.concatenate([lse_s[2 * i], lse_s[2 * i + 1]], axis=0) for i in range(tiles)], axis=1
    )
    hi = lse.astype(BF16).astype(F32)
    mid = (lse - hi).astype(BF16).astype(F32)
    lo = lse - hi - mid
    stats = jnp.concatenate([hi, mid, lo, jnp.zeros_like(hi)], axis=0)
    stats = jnp.concatenate([stats, jnp.zeros((8, LANES), F32)], axis=1)
    blocks = out_ref.shape[0]
    rows = n_q // blocks
    for b in range(blocks):
        out_ref[b, :rows] = o_s[b * rows : (b + 1) * rows]
        for k in range(STAT_ROWS // 8):
            at = b * rows + k * LANES
            out_ref[b, rows + 8 * k : rows + 8 * k + 8] = stats[:, at : at + LANES].astype(BF16)


def combine_kernel(part_ref, ga_ref, gated_b_ref, wa_ref, wb_ref, out_ref):
    blocks, padded, _ = part_ref.shape
    rows = padded - STAT_ROWS
    lses = []
    for s in range(blocks):
        pieces = [
            part_ref[s, rows + 8 * k : rows + 8 * k + 8].astype(F32) for k in range(STAT_ROWS // 8)
        ]
        x = jnp.concatenate(pieces, axis=1)
        lses.append(x[0:2] + x[2:4] + x[4:6])
    top = functools.reduce(jnp.maximum, lses)
    weights = [jnp.exp(v - top) for v in lses]
    den = functools.reduce(jnp.add, weights)
    stacked = jnp.concatenate([v / den for v in weights], axis=0)
    cols = jnp.concatenate(
        [stacked, jnp.zeros((LANES - 2 * blocks, stacked.shape[1]), F32)], axis=0
    ).T
    low = lax.broadcasted_iota(jnp.int32, (rows, LANES), 1) < HEAD
    acc = jnp.zeros((rows, LANES), F32)
    for s in range(blocks):
        w = jnp.where(low, cols[:rows, 2 * s : 2 * s + 1], cols[:rows, 2 * s + 1 : 2 * s + 2])
        acc = acc + w * part_ref[s, :rows].astype(F32)
    gated_a = (acc * silu(ga_ref[...].astype(F32))).astype(BF16)
    gated = jnp.concatenate([gated_a, gated_b_ref[...]], axis=1)
    w = jnp.concatenate([wa_ref[...], wb_ref[...]], axis=0)
    out_ref[...] = dot(gated, w).astype(BF16)


def call(kernel, outs, scratch, smem, *args, name, flops=0):
    specs = [
        pl.BlockSpec(memory_space=pltpu.SMEM if i in smem else pltpu.VMEM)
        for i in range(len(args))
    ]
    return pl.pallas_call(
        kernel,
        out_shape=outs,
        in_specs=specs,
        out_specs=jax.tree.map(lambda _: pl.BlockSpec(memory_space=pltpu.VMEM), outs),
        scratch_shapes=scratch,
        compiler_params=pltpu.CompilerParams(vmem_limit_bytes=56 * 2**20),
        cost_estimate=pl.CostEstimate(flops=flops, bytes_accessed=2**20, transcendentals=0),
        name=name,
    )(*args)


def shaped(*shape, dtype=BF16):
    return jax.ShapeDtypeStruct(shape, dtype)


def body(
    tokens, norm_gain, w_qa, w_ka, w_va, qgain_a, kgain_a, w_qb, w_kb, w_vb, sink_b, w_ga, w_gb,
    out_a, out_b,
):
    rows, width = tokens.shape
    n_z, n_y, n_x = (lax.axis_size(a) for a in ("z", "y", "x"))
    blocks = n_z * n_y
    tp = 2 * n_x
    s_index = lax.axis_index("z") * n_y + lax.axis_index("y")
    core = lax.axis_index("core")
    row_table, col_table = rotary_tables(blocks * rows)
    grid_rows = rows // GRID
    row_here = lax.dynamic_slice_in_dim(jnp.asarray(row_table), s_index * grid_rows, grid_rows, 1)

    mine = lax.all_gather(tokens, "x", axis=0)
    other = lax.ppermute(mine, "core", [(0, 1), (1, 0)])
    kgain = jnp.concatenate([kgain_a, jnp.zeros_like(kgain_a)], axis=1)
    q8, kv, qb, kvb, ga, gb = call(
        project_kernel,
        (shaped(n_y, rows, LANES), *(shaped(rows, LANES) for _ in range(5))),
        [pltpu.VMEM((tp, rows, width), BF16)],
        {0},
        core.reshape(1).astype(jnp.int32), mine, other, norm_gain.reshape(tp, 1, width),
        w_qa, w_ka, w_va, w_qb, w_kb, w_vb, w_ga, w_gb,
        qgain_a.reshape(1, LANES), kgain, row_here, jnp.asarray(col_table),
        name="project", flops=2 * rows * width * tp * 768,
    )
    q_all = lax.all_to_all(q8, "y", 0, 0, tiled=True)
    kv_all = lax.all_gather(kv, "z", axis=0, tiled=True)
    up = [(i, i + 1) for i in range(blocks - 1)]
    down = [(i + 1, i) for i in range(blocks - 1)]
    before = lax.ppermute(kvb[rows - WINDOW :], ("z", "y"), up)
    after = lax.ppermute(kvb[:WINDOW], ("z", "y"), down)
    gated_b = call(
        window_kernel,
        shaped(rows, LANES),
        [],
        {0, 5},
        jnp.stack([s_index, jnp.int32(blocks)]).astype(jnp.int32), qb, kvb, before, after,
        sink_b, gb,
        name="windowed", flops=4 * 2 * rows * 576 * 64,
    )
    n_q = n_y * rows
    n_k = n_z * rows
    tile = 512
    parts = call(
        functools.partial(attend_kernel, tile=tile, chunk=256),
        shaped(n_y, rows + STAT_ROWS, LANES),
        [
            pltpu.VMEM((n_k, LANES), BF16),
            pltpu.VMEM((ACC_ROWS, n_k), BF16),
            pltpu.VMEM((2 * n_q // tile, LANES, tile), BF16),
            pltpu.VMEM((2 * n_q // tile, 1, tile), F32),
            pltpu.VMEM((n_q, LANES), BF16),
            pltpu.VMEM((2 * n_q // tile, 1, tile), F32),
        ],
        {},
        q_all.reshape(n_q, LANES), kv_all,
        name="attend", flops=4 * 2 * n_q * n_k * 64,
    )
    back = lax.all_to_all(parts, "y", 0, 0, tiled=True)
    partial = call(
        combine_kernel,
        shaped(rows, out_a.shape[1]),
        [],
        {},
        back, ga, gated_b, out_a, out_b,
        name="combine", flops=2 * rows * 256 * 2048,
    )
    by_place = partial.reshape(n_x, 2, rows // tp, out_a.shape[1])
    sent = lax.dynamic_index_in_dim(by_place, 1 - core, 1, keepdims=False)
    kept = lax.dynamic_index_in_dim(by_place, core, 1, keepdims=False)
    got = lax.ppermute(sent, "core", [(0, 1), (1, 0)])
    paired = (kept.astype(F32) + got.astype(F32)).astype(BF16)
    arrived = lax.all_to_all(paired, "x", 0, 0, tiled=True)
    return jnp.sum(arrived.astype(F32), axis=0).astype(BF16)


def solution(mesh):
    n_sp, n_tp = (mesh.shape["sp"], mesh.shape["tp"])
    n_z = 8
    fine = Mesh(
        np.asarray(mesh.devices).reshape(n_z, n_sp // n_z, n_tp // 2, 2), ("z", "y", "x", "core")
    )
    sp = ("z", "y")
    tp = ("x", "core")
    placed = (
        P(sp, tp), P(), P(None, tp), P(None, tp), P(None, tp), P(tp, None), P(tp, None),
        P(None, tp), P(None, tp), P(None, tp), P(tp), P(None, tp), P(None, tp), P(tp, None),
        P(tp, None),
    )
    return jax.shard_map(
        body, mesh=fine, in_specs=placed, out_specs=P((*sp, *tp), None), check_vma=False
    )
```

```python
import functools

import jax
import jax.numpy as jnp
import numpy as np
from jax import lax
from jax.experimental import pallas as pl
from jax.experimental.pallas import tpu as pltpu
from jax.sharding import Mesh, PartitionSpec as P

GRID = 64
WINDOW = 128
EPSILON = 1e-06
THETA = 10000.0
HEAD = 64
LANES = 128
BOUND = 69.0
SHIFT = 55.0
STAT_ROWS = 24
ACC_ROWS = 80
F32 = jnp.float32
BF16 = jnp.bfloat16


def rotary_tables(seq):
    quarter = HEAD // 4
    freq = np.power(np.float32(THETA), -np.arange(quarter, dtype=np.float32) / np.float32(quarter))
    freq = freq.astype(np.float32)

    def table(count, which):
        angle = (np.arange(count, dtype=np.float32)[:, None] * freq).astype(np.float64)
        out = []
        for fn in (np.cos, np.sin):
            half = np.concatenate([fn(angle), fn(angle)], axis=1)
            zero = np.zeros_like(half)
            head = np.concatenate([half, zero] if which == 0 else [zero, half], axis=1)
            out.append(np.concatenate([head, head], axis=1).astype(np.float32))
        return np.stack(out)

    return table(seq // GRID, 0), table(GRID, 1)


def dot(a, b):
    return jnp.dot(a, b, preferred_element_type=F32)


def dot_t(a, b):
    return lax.dot_general(a, b, (((1,), (1,)), ((), ())), preferred_element_type=F32)


def silu(v):
    return v / (1.0 + jnp.exp(-v))


def project_kernel(
    place_ref, mine_ref, other_ref, gain_ref, qgain_ref, kgain_ref, row_ref, col_ref,
    wqa, wka, wva, wqb, wkb, wvb, wga, wgb,
    q_out, kv_out, qb_out, kvb_out, first_out, last_out, ga_out, gb_out,
    h_s, wide_s, narrow_s, sems,
):
    wide = [wqa, wqb, wga, wgb]
    narrow = [wka, wva, wkb, wvb]
    copies = [
        pltpu.make_async_copy(ref, narrow_s.at[i * HEAD : (i + 1) * HEAD], sems.at[i])
        for i, ref in enumerate(narrow)
    ]
    copies += [
        pltpu.make_async_copy(ref, wide_s.at[i], sems.at[4 + i]) for i, ref in enumerate(wide)
    ]
    for copy in copies:
        copy.start()
    core = place_ref[0]
    s_index = place_ref[1]
    chips, rows, width = mine_ref.shape
    total = jnp.zeros((rows, 1), F32)
    for ref in (mine_ref, other_ref):
        for i in range(chips):
            part = ref[i].astype(F32)
            total = total + jnp.sum(part * part, axis=1, keepdims=True)
    scale = lax.rsqrt(total / (2 * chips * width) + EPSILON)
    for ref, side in ((mine_ref, core), (other_ref, 1 - core)):
        for i in range(chips):
            t = 2 * i + side
            h_s[t] = (ref[i].astype(F32) * scale * gain_ref[t]).astype(BF16)
    normed = jnp.concatenate([h_s[t] for t in range(2 * chips)], axis=1)
    for copy in copies:
        copy.wait()
    both_kv = dot_t(normed, narrow_s[...])
    both_q = dot(normed, jnp.concatenate([wide_s[0], wide_s[1]], axis=1))
    both_g = dot(normed, jnp.concatenate([wide_s[2], wide_s[3]], axis=1))
    ga_out[...] = both_g[:, :LANES].astype(BF16)
    gb_out[...] = both_g[:, LANES:].astype(BF16)
    qb_out[...] = both_q[:, LANES:].astype(BF16)
    kvb = both_kv[:, LANES:].astype(BF16)
    kvb_out[...] = kvb
    first_out[...] = kvb[:WINDOW]
    last_out[...] = kvb[rows - WINDOW :]
    cos = []
    sin = []
    grid_rows = rows // GRID
    for r in range(grid_rows):
        at = s_index * grid_rows + r
        cos.append(row_ref[0, pl.ds(at, 1), :] + col_ref[0])
        sin.append(row_ref[1, pl.ds(at, 1), :] + col_ref[1])
    cos = jnp.concatenate(cos, axis=0)
    sin = jnp.concatenate(sin, axis=0)
    lane = lax.broadcasted_iota(jnp.int32, (rows, LANES), 1)
    first = (lane % 32) < 16
    low = lane < HEAD

    def turned(n):
        partner = jnp.where(first, -pltpu.roll(n, LANES - 16, 1), pltpu.roll(n, 16, 1))
        return n * cos + partner * sin

    v = both_q[:, :LANES].astype(BF16).astype(F32)
    square = v * v
    sum_low = jnp.sum(jnp.where(low, square, 0.0), axis=1, keepdims=True)
    sum_high = jnp.sum(jnp.where(low, 0.0, square), axis=1, keepdims=True)
    rs_low = lax.rsqrt(sum_low / HEAD + EPSILON)
    rs_high = lax.rsqrt(sum_high / HEAD + EPSILON)
    qgain = jnp.concatenate([qgain_ref[0:1, :], qgain_ref[1:2, :]], axis=1)
    q_out[...] = turned(v * jnp.where(low, rs_low, rs_high) * qgain).astype(BF16)
    kv = both_kv[:, :LANES].astype(BF16).astype(F32)
    k_only = jnp.where(low, kv, 0.0)
    sq = jnp.sum(k_only * k_only, axis=1, keepdims=True)
    kgain = jnp.concatenate([kgain_ref[...], kgain_ref[...]], axis=1)
    ka = turned(k_only * lax.rsqrt(sq / HEAD + EPSILON) * kgain)
    both = jnp.where(low, ka, kv).astype(BF16)
    for i in range(kv_out.shape[0]):
        kv_out[i] = both


def window_kernel(
    place_ref, q_ref, mid_ref, prev_ref, next_ref, sink_ref, gate_ref, out_ref, *, count
):
    s_index = place_ref[1]
    rows = q_ref.shape[0]
    kv = jnp.concatenate([prev_ref[...], mid_ref[...], next_ref[...]], axis=0)
    span = kv.shape[0]
    r = lax.broadcasted_iota(jnp.int32, (rows, span), 0)
    c = lax.broadcasted_iota(jnp.int32, (rows, span), 1)
    place = s_index * rows - WINDOW + c
    allowed = (c >= r) & (c - r <= 2 * WINDOW) & (place >= 0) & (place < rows * count)
    keys = kv[:, :HEAD]
    values = kv[:, HEAD:]
    outs = []
    for h in range(2):
        s = dot_t(q_ref[:, h * HEAD : (h + 1) * HEAD], keys) * HEAD ** (-0.5)
        s = jnp.where(allowed, s, -1e30)
        sink = sink_ref[h]
        top = jnp.maximum(jnp.max(s, axis=1, keepdims=True), sink)
        p = jnp.where(allowed, jnp.exp(s - top), 0.0)
        den = jnp.sum(p, axis=1, keepdims=True) + jnp.exp(sink - top)
        outs.append(dot(p.astype(BF16), values) / den)
    att = jnp.concatenate(outs, axis=1)
    out_ref[...] = (att * silu(gate_ref[...].astype(F32))).astype(BF16)


def attend_kernel(
    q_ref, kv_ref, out_ref, k_s, vt_s, qt_s, m_s, o_s, lse_s, p_s, *, tile, chunk
):
    n_q = q_ref.shape[0]
    n_k = kv_ref.shape[0]
    tiles = n_q // tile
    steps = 2 * tiles
    chunks = n_k // chunk
    kv = kv_ref[...]
    lane = lax.broadcasted_iota(jnp.int32, (n_k, LANES), 1)
    ones = jnp.where(lane < HEAD + 3, 1.0, 0.0)
    k_s[...] = jnp.where(lane < HEAD, kv.astype(F32), ones).astype(BF16)
    kv_t = kv.astype(F32).T
    k_t = kv_t[:HEAD]
    k_norm = jnp.max(jnp.sum(k_t * k_t, axis=0, keepdims=True))
    row16 = lax.broadcasted_iota(jnp.int32, (ACC_ROWS - HEAD, chunk), 0)
    for c in range(chunks):
        vt_s[c, :HEAD] = kv_t[HEAD:, c * chunk : (c + 1) * chunk].astype(BF16)
        vt_s[c, HEAD:] = jnp.where(row16 == 0, 1.0, 0.0).astype(BF16)
    top = jnp.float32(0.0)
    for i in range(tiles):
        q_t = q_ref[i * tile : (i + 1) * tile, :].astype(F32).T
        for h in range(2):
            part = q_t[h * HEAD : (h + 1) * HEAD] * HEAD ** (-0.5)
            bound = jnp.sqrt(jnp.sum(part * part, axis=0, keepdims=True) * k_norm) * 1.0001
            top = jnp.maximum(top, jnp.max(bound))
            m_s[2 * i + h] = bound - SHIFT
            qt_s[2 * i + h, :HEAD] = part.astype(BF16)
            qt_s[2 * i + h, HEAD:] = jnp.zeros((LANES - HEAD, tile), BF16)

    @pl.when(top > BOUND)
    def _():
        def row_max(t, carry):
            def one(c, m):
                s = dot(k_s[pl.ds(pl.multiple_of(c * chunk, chunk), chunk), :], qt_s[t])
                return jnp.maximum(m, jnp.max(s, axis=0, keepdims=True))

            m_s[t] = lax.fori_loop(0, chunks, one, jnp.full((1, tile), -1e30, F32))
            return carry

        lax.fori_loop(0, steps, row_max, 0)

    row = lax.broadcasted_iota(jnp.int32, (16, tile), 0)
    for t in range(steps):
        neg = -m_s[t]
        hi = neg.astype(BF16).astype(F32)
        mid = (neg - hi).astype(BF16).astype(F32)
        lo = neg - hi - mid
        parts = jnp.where(row == 0, hi, jnp.where(row == 1, mid, jnp.where(row == 2, lo, 0.0)))
        qt_s[t, HEAD : HEAD + 16] = parts.astype(BF16)

    def both(ahead, ahead_slot, now, now_slot):
        if ahead is not None:
            q_here = qt_s[ahead]
        acc = jnp.zeros((ACC_ROWS, tile), F32)
        for c in range(chunks):
            if ahead is not None:
                s = dot(k_s[c * chunk : (c + 1) * chunk, :], q_here)
                p_s[ahead_slot, c] = jnp.exp(s).astype(BF16)
            if now is not None:
                acc = acc + dot(vt_s[c], p_s[now_slot, c])
        if now is not None:
            total = acc[HEAD : HEAD + 1]
            lse_s[now] = m_s[now] + jnp.log(total)
            o_s[now] = acc[:HEAD] / total

    both(0, 0, None, None)

    def pair(n, carry):
        both(2 * n + 1, 1, 2 * n, 0)
        both(2 * n + 2, 0, 2 * n + 1, 1)
        return carry

    lax.fori_loop(0, (steps - 2) // 2, pair, 0)
    both(steps - 1, 1, steps - 2, 0)
    both(None, None, steps - 1, 1)

    lse = jnp.concatenate(
        [jnp.concatenate([lse_s[2 * i], lse_s[2 * i + 1]], axis=0) for i in range(tiles)], axis=1
    )
    hi = lse.astype(BF16).astype(F32)
    mid = (lse - hi).astype(BF16).astype(F32)
    lo = lse - hi - mid
    stats = jnp.concatenate([hi, mid, lo, jnp.zeros_like(hi)], axis=0)
    stats = jnp.concatenate([stats, jnp.zeros((8, LANES), F32)], axis=1)
    blocks = out_ref.shape[0]
    rows = n_q // blocks
    flat = jnp.concatenate(
        [
            jnp.concatenate([o_s[2 * i], o_s[2 * i + 1]], axis=0).T.astype(BF16)
            for i in range(tiles)
        ],
        axis=0,
    )
    for b in range(blocks):
        out_ref[b, :rows] = flat[b * rows : (b + 1) * rows]
        for k in range(STAT_ROWS // 8):
            at = b * rows + k * LANES
            out_ref[b, rows + 8 * k : rows + 8 * k + 8] = stats[:, at : at + LANES].astype(BF16)


def combine_kernel(
    place_ref, part_ref, ga_ref, gated_b_ref, wa_ref, wb_ref, kept_ref, sent_ref, out_s
):
    blocks, padded, _ = part_ref.shape
    rows = padded - STAT_ROWS
    lses = []
    for s in range(blocks):
        pieces = [
            part_ref[s, rows + 8 * k : rows + 8 * k + 8].astype(F32) for k in range(STAT_ROWS // 8)
        ]
        x = jnp.concatenate(pieces, axis=1)
        lses.append(x[0:2] + x[2:4] + x[4:6])
    top = functools.reduce(jnp.maximum, lses)
    weights = [jnp.exp(v - top) for v in lses]
    den = functools.reduce(jnp.add, weights)
    stacked = jnp.concatenate([v / den for v in weights], axis=0)
    cols = jnp.concatenate(
        [stacked, jnp.zeros((LANES - 2 * blocks, stacked.shape[1]), F32)], axis=0
    ).T
    low = lax.broadcasted_iota(jnp.int32, (rows, LANES), 1) < HEAD
    acc = jnp.zeros((rows, LANES), F32)
    for s in range(blocks):
        w = jnp.where(low, cols[:rows, 2 * s : 2 * s + 1], cols[:rows, 2 * s + 1 : 2 * s + 2])
        acc = acc + w * part_ref[s, :rows].astype(F32)
    gated_a = (acc * silu(ga_ref[...].astype(F32))).astype(BF16)
    gated = jnp.concatenate([gated_a, gated_b_ref[...]], axis=1)
    w = jnp.concatenate([wa_ref[...], wb_ref[...]], axis=0)
    result = dot(gated, w).astype(BF16)
    core = place_ref[0]
    chips, piece, _ = kept_ref.shape
    for t in range(2 * chips):
        out_s[t] = result[t * piece : (t + 1) * piece]
    for i in range(chips):
        kept_ref[i] = out_s[2 * i + core]
        sent_ref[i] = out_s[2 * i + 1 - core]


def call(kernel, outs, scratch, smem, near, *args, name, flops=0, far=()):
    args = [
        pltpu.with_memory_space_constraint(a, pltpu.VMEM) if i in near else a
        for i, a in enumerate(args)
    ]
    specs = [
        pl.BlockSpec(
            memory_space=pltpu.SMEM if i in smem else pl.ANY if i in far else pltpu.VMEM
        )
        for i in range(len(args))
    ]
    return pl.pallas_call(
        kernel,
        out_shape=outs,
        in_specs=specs,
        out_specs=jax.tree.map(lambda _: pl.BlockSpec(memory_space=pltpu.VMEM), outs),
        scratch_shapes=scratch,
        compiler_params=pltpu.CompilerParams(vmem_limit_bytes=56 * 2**20),
        cost_estimate=pl.CostEstimate(flops=flops, bytes_accessed=2**20, transcendentals=0),
        name=name,
    )(*args)


def shaped(*shape, dtype=BF16):
    return jax.ShapeDtypeStruct(shape, dtype)


def body(
    tokens, norm_gain, w_qa, w_ka, w_va, qgain_a, kgain_a, w_qb, w_kb, w_vb, sink_b, w_ga, w_gb,
    out_a, out_b,
):
    rows, width = tokens.shape
    n_z, n_y, n_x = (lax.axis_size(a) for a in ("z", "y", "x"))
    blocks = n_z * n_y
    tp = 2 * n_x
    s_index = lax.axis_index("z") * n_y + lax.axis_index("y")
    core = lax.axis_index("core")
    place = jnp.stack([core, s_index]).astype(jnp.int32)
    row_table, col_table = rotary_tables(blocks * rows)

    mine = lax.all_gather(tokens, "x", axis=0)
    other = lax.ppermute(mine, "core", [(0, 1), (1, 0)])
    q, kv8, qb, kvb, kvb_first, kvb_last, ga, gb = call(
        project_kernel,
        (
            shaped(rows, LANES), shaped(n_z, rows, LANES),
            shaped(rows, LANES), shaped(rows, LANES),
            shaped(WINDOW, LANES), shaped(WINDOW, LANES),
            shaped(rows, LANES), shaped(rows, LANES),
        ),
        [
            pltpu.VMEM((tp, rows, width), BF16),
            pltpu.VMEM((4, tp * width, LANES), BF16),
            pltpu.VMEM((4 * HEAD, tp * width), BF16),
            pltpu.SemaphoreType.DMA((8,)),
        ],
        {0},
        {1, 2},
        place, mine, other, norm_gain.reshape(tp, 1, width), qgain_a, kgain_a,
        jnp.asarray(row_table), jnp.asarray(col_table),
        w_qa, w_ka.T, w_va.T, w_qb, w_kb.T, w_vb.T, w_ga, w_gb,
        name="project", flops=2 * rows * width * tp * 768, far=set(range(8, 16)),
    )
    kv_all = lax.all_to_all(kv8, "z", 0, 0, tiled=True)
    q_all = lax.all_gather(q, "y", axis=0, tiled=True)
    up = [(i, i + 1) for i in range(blocks - 1)]
    down = [(i + 1, i) for i in range(blocks - 1)]
    before = lax.ppermute(kvb_last, ("z", "y"), up)
    after = lax.ppermute(kvb_first, ("z", "y"), down)
    gated_b = call(
        functools.partial(window_kernel, count=blocks),
        shaped(rows, LANES),
        [],
        {0, 5},
        {3, 4},
        place, qb, kvb, before, after, sink_b, gb,
        name="windowed", flops=4 * 2 * rows * 576 * 64,
    )
    n_q = n_y * rows
    n_k = n_z * rows
    tile = 512
    chunk = 256
    steps = 2 * n_q // tile
    parts = call(
        functools.partial(attend_kernel, tile=tile, chunk=chunk),
        shaped(n_y, rows + STAT_ROWS, LANES),
        [
            pltpu.VMEM((n_k, LANES), BF16),
            pltpu.VMEM((n_k // chunk, ACC_ROWS, chunk), BF16),
            pltpu.VMEM((steps, LANES, tile), BF16),
            pltpu.VMEM((steps, 1, tile), F32),
            pltpu.VMEM((steps, HEAD, tile), F32),
            pltpu.VMEM((steps, 1, tile), F32),
            pltpu.VMEM((2, n_k // chunk, chunk, tile), BF16),
        ],
        {},
        {0, 1},
        q_all, kv_all.reshape(n_k, LANES),
        name="attend", flops=4 * 2 * n_q * n_k * 64,
    )
    back = lax.all_to_all(parts, "y", 0, 0, tiled=True)
    piece = shaped(n_x, rows // tp, out_a.shape[1])
    kept, sent = call(
        combine_kernel,
        (piece, piece),
        [pltpu.VMEM((tp, rows // tp, out_a.shape[1]), BF16)],
        {0},
        {1, 4, 5},
        place, back, ga, gated_b, out_a, out_b,
        name="combine", flops=2 * rows * 256 * 2048,
    )
    got = lax.ppermute(sent, "core", [(0, 1), (1, 0)])
    paired = (kept.astype(F32) + got.astype(F32)).astype(BF16)
    arrived = lax.all_to_all(paired, "x", 0, 0, tiled=True)
    return jnp.sum(arrived.astype(F32), axis=0).astype(BF16)


def solution(mesh):
    n_sp, n_tp = (mesh.shape["sp"], mesh.shape["tp"])
    n_z = 8
    fine = Mesh(
        np.asarray(mesh.devices).reshape(n_z, n_sp // n_z, n_tp // 2, 2), ("z", "y", "x", "core")
    )
    sp = ("z", "y")
    tp = ("x", "core")
    placed = (
        P(sp, tp), P(), P(None, tp), P(None, tp), P(None, tp), P(tp, None), P(tp, None),
        P(None, tp), P(None, tp), P(None, tp), P(tp), P(None, tp), P(None, tp), P(tp, None),
        P(tp, None),
    )
    return jax.shard_map(
        body, mesh=fine, in_specs=placed, out_specs=P((*sp, *tp), None), check_vma=False
    )
```

```python
import functools

import jax
import jax.numpy as jnp
import numpy as np
from jax import lax
from jax.experimental import pallas as pl
from jax.experimental.pallas import tpu as pltpu
from jax.sharding import Mesh, PartitionSpec as P

GRID = 64
WINDOW = 128
EPSILON = 1e-06
THETA = 10000.0
HEAD = 64
LANES = 128
BOUND = 69.0
SHIFT = 55.0
STAT_ROWS = 24
ACC_ROWS = 80
SP = ("zh", "zl", "yh", "yl")
TP = ("x", "core")
Q_GROUP = ("yl", "zl")
K_GROUP = ("zh", "yh")
F32 = jnp.float32
BF16 = jnp.bfloat16


def rotary_tables(seq):
    quarter = HEAD // 4
    freq = np.power(np.float32(THETA), -np.arange(quarter, dtype=np.float32) / np.float32(quarter))
    freq = freq.astype(np.float32)

    def table(count, which):
        angle = (np.arange(count, dtype=np.float32)[:, None] * freq).astype(np.float64)
        out = []
        for fn in (np.cos, np.sin):
            half = np.concatenate([fn(angle), fn(angle)], axis=1)
            zero = np.zeros_like(half)
            head = np.concatenate([half, zero] if which == 0 else [zero, half], axis=1)
            out.append(np.concatenate([head, head], axis=1).astype(np.float32))
        return np.stack(out)

    return table(seq // GRID, 0), table(GRID, 1)


def dot(a, b):
    return jnp.dot(a, b, preferred_element_type=F32)


def dot_t(a, b):
    return lax.dot_general(a, b, (((1,), (1,)), ((), ())), preferred_element_type=F32)


def silu(v):
    return v / (1.0 + jnp.exp(-v))


def project_kernel(
    place_ref, mine_ref, other_ref, gain_ref, qgain_ref, kgain_ref, row_ref, col_ref,
    wqa, wka, wva, wqb, wkb, wvb, wga, wgb,
    q_out, kv_out, qb_out, kvb_out, first_out, last_out, ga_out, gb_out,
    h_s, wide_s, narrow_s, sems,
):
    wide = [wqa, wqb, wga, wgb]
    narrow = [wka, wva, wkb, wvb]
    copies = [
        pltpu.make_async_copy(ref, narrow_s.at[i * HEAD : (i + 1) * HEAD], sems.at[i])
        for i, ref in enumerate(narrow)
    ]
    copies += [
        pltpu.make_async_copy(ref, wide_s.at[i], sems.at[4 + i]) for i, ref in enumerate(wide)
    ]
    for copy in copies:
        copy.start()
    core = place_ref[0]
    s_index = place_ref[1]
    chips, rows, width = mine_ref.shape
    total = jnp.zeros((rows, 1), F32)
    for ref in (mine_ref, other_ref):
        for i in range(chips):
            part = ref[i].astype(F32)
            total = total + jnp.sum(part * part, axis=1, keepdims=True)
    scale = lax.rsqrt(total / (2 * chips * width) + EPSILON)
    for ref, side in ((mine_ref, core), (other_ref, 1 - core)):
        for i in range(chips):
            t = 2 * i + side
            h_s[t] = (ref[i].astype(F32) * scale * gain_ref[t]).astype(BF16)
    normed = jnp.concatenate([h_s[t] for t in range(2 * chips)], axis=1)
    for copy in copies:
        copy.wait()
    both_kv = dot_t(normed, narrow_s[...])
    both_q = dot(normed, jnp.concatenate([wide_s[0], wide_s[1]], axis=1))
    both_g = dot(normed, jnp.concatenate([wide_s[2], wide_s[3]], axis=1))
    ga_out[...] = both_g[:, :LANES].astype(BF16)
    gb_out[...] = both_g[:, LANES:].astype(BF16)
    qb_out[...] = both_q[:, LANES:].astype(BF16)
    kvb = both_kv[:, LANES:].astype(BF16)
    kvb_out[...] = kvb
    first_out[...] = kvb[:WINDOW]
    last_out[...] = kvb[rows - WINDOW :]
    cos = []
    sin = []
    grid_rows = rows // GRID
    for r in range(grid_rows):
        at = s_index * grid_rows + r
        cos.append(row_ref[0, pl.ds(at, 1), :] + col_ref[0])
        sin.append(row_ref[1, pl.ds(at, 1), :] + col_ref[1])
    cos = jnp.concatenate(cos, axis=0)
    sin = jnp.concatenate(sin, axis=0)
    lane = lax.broadcasted_iota(jnp.int32, (rows, LANES), 1)
    first = (lane % 32) < 16
    low = lane < HEAD

    def turned(n):
        partner = jnp.where(first, -pltpu.roll(n, LANES - 16, 1), pltpu.roll(n, 16, 1))
        return n * cos + partner * sin

    v = both_q[:, :LANES].astype(BF16).astype(F32)
    square = v * v
    sum_low = jnp.sum(jnp.where(low, square, 0.0), axis=1, keepdims=True)
    sum_high = jnp.sum(jnp.where(low, 0.0, square), axis=1, keepdims=True)
    rs_low = lax.rsqrt(sum_low / HEAD + EPSILON)
    rs_high = lax.rsqrt(sum_high / HEAD + EPSILON)
    qgain = jnp.concatenate([qgain_ref[0:1, :], qgain_ref[1:2, :]], axis=1)
    q_out[...] = turned(v * jnp.where(low, rs_low, rs_high) * qgain).astype(BF16)
    kv = both_kv[:, :LANES].astype(BF16).astype(F32)
    k_only = jnp.where(low, kv, 0.0)
    sq = jnp.sum(k_only * k_only, axis=1, keepdims=True)
    kgain = jnp.concatenate([kgain_ref[...], kgain_ref[...]], axis=1)
    ka = turned(k_only * lax.rsqrt(sq / HEAD + EPSILON) * kgain)
    both = jnp.where(low, ka, kv).astype(BF16)
    for i in range(kv_out.shape[0]):
        kv_out[i] = both


def window_kernel(
    place_ref, q_ref, mid_ref, prev_ref, next_ref, sink_ref, gate_ref, out_ref, *, count
):
    s_index = place_ref[1]
    rows = q_ref.shape[0]
    kv = jnp.concatenate([prev_ref[...], mid_ref[...], next_ref[...]], axis=0)
    span = kv.shape[0]
    r = lax.broadcasted_iota(jnp.int32, (rows, span), 0)
    c = lax.broadcasted_iota(jnp.int32, (rows, span), 1)
    place = s_index * rows - WINDOW + c
    allowed = (c >= r) & (c - r <= 2 * WINDOW) & (place >= 0) & (place < rows * count)
    keys = kv[:, :HEAD]
    values = kv[:, HEAD:]
    outs = []
    for h in range(2):
        s = dot_t(q_ref[:, h * HEAD : (h + 1) * HEAD], keys) * HEAD ** (-0.5)
        s = jnp.where(allowed, s, -1e30)
        sink = sink_ref[h]
        top = jnp.maximum(jnp.max(s, axis=1, keepdims=True), sink)
        p = jnp.where(allowed, jnp.exp(s - top), 0.0)
        den = jnp.sum(p, axis=1, keepdims=True) + jnp.exp(sink - top)
        outs.append(dot(p.astype(BF16), values) / den)
    att = jnp.concatenate(outs, axis=1)
    out_ref[...] = (att * silu(gate_ref[...].astype(F32))).astype(BF16)


def attend_kernel(
    q_ref, kv_ref, out_ref, k_s, vt_s, qt_s, m_s, o_s, lse_s, p_s, *, tile, chunk
):
    n_q = q_ref.shape[0]
    n_k = kv_ref.shape[0]
    tiles = n_q // tile
    steps = 2 * tiles
    chunks = n_k // chunk
    kv = kv_ref[...]
    lane = lax.broadcasted_iota(jnp.int32, (n_k, LANES), 1)
    ones = jnp.where(lane < HEAD + 3, 1.0, 0.0)
    k_s[...] = jnp.where(lane < HEAD, kv.astype(F32), ones).astype(BF16)
    kv_t = kv.astype(F32).T
    k_t = kv_t[:HEAD]
    k_norm = jnp.max(jnp.sum(k_t * k_t, axis=0, keepdims=True))
    row16 = lax.broadcasted_iota(jnp.int32, (ACC_ROWS - HEAD, chunk), 0)
    for c in range(chunks):
        vt_s[c, :HEAD] = kv_t[HEAD:, c * chunk : (c + 1) * chunk].astype(BF16)
        vt_s[c, HEAD:] = jnp.where(row16 == 0, 1.0, 0.0).astype(BF16)
    top = jnp.float32(0.0)
    for i in range(tiles):
        q_t = q_ref[i * tile : (i + 1) * tile, :].astype(F32).T
        for h in range(2):
            part = q_t[h * HEAD : (h + 1) * HEAD] * HEAD ** (-0.5)
            bound = jnp.sqrt(jnp.sum(part * part, axis=0, keepdims=True) * k_norm) * 1.0001
            top = jnp.maximum(top, jnp.max(bound))
            m_s[2 * i + h] = bound - SHIFT
            qt_s[2 * i + h, :HEAD] = part.astype(BF16)
            qt_s[2 * i + h, HEAD:] = jnp.zeros((LANES - HEAD, tile), BF16)

    @pl.when(top > BOUND)
    def _():
        def row_max(t, carry):
            def one(c, m):
                s = dot(k_s[pl.ds(pl.multiple_of(c * chunk, chunk), chunk), :], qt_s[t])
                return jnp.maximum(m, jnp.max(s, axis=0, keepdims=True))

            m_s[t] = lax.fori_loop(0, chunks, one, jnp.full((1, tile), -1e30, F32))
            return carry

        lax.fori_loop(0, steps, row_max, 0)

    row = lax.broadcasted_iota(jnp.int32, (16, tile), 0)
    for t in range(steps):
        neg = -m_s[t]
        hi = neg.astype(BF16).astype(F32)
        mid = (neg - hi).astype(BF16).astype(F32)
        lo = neg - hi - mid
        parts = jnp.where(row == 0, hi, jnp.where(row == 1, mid, jnp.where(row == 2, lo, 0.0)))
        qt_s[t, HEAD : HEAD + 16] = parts.astype(BF16)

    def both(ahead, ahead_slot, now, now_slot):
        if ahead is not None:
            q_here = qt_s[ahead]
        acc = jnp.zeros((ACC_ROWS, tile), F32)
        for c in range(chunks):
            if ahead is not None:
                s = dot(k_s[c * chunk : (c + 1) * chunk, :], q_here)
                p_s[ahead_slot, c] = jnp.exp(s).astype(BF16)
            if now is not None:
                acc = acc + dot(vt_s[c], p_s[now_slot, c])
        if now is not None:
            total = acc[HEAD : HEAD + 1]
            lse_s[now] = m_s[now] + jnp.log(total)
            o_s[now] = acc[:HEAD] / total

    both(0, 0, None, None)

    def pair(n, carry):
        both(2 * n + 1, 1, 2 * n, 0)
        both(2 * n + 2, 0, 2 * n + 1, 1)
        return carry

    lax.fori_loop(0, (steps - 2) // 2, pair, 0)
    both(steps - 1, 1, steps - 2, 0)
    both(None, None, steps - 1, 1)

    lse = jnp.concatenate(
        [jnp.concatenate([lse_s[2 * i], lse_s[2 * i + 1]], axis=0) for i in range(tiles)], axis=1
    )
    hi = lse.astype(BF16).astype(F32)
    mid = (lse - hi).astype(BF16).astype(F32)
    lo = lse - hi - mid
    stats = jnp.concatenate([hi, mid, lo, jnp.zeros_like(hi)], axis=0)
    stats = jnp.concatenate([stats, jnp.zeros((8, LANES), F32)], axis=1)
    blocks = out_ref.shape[0]
    rows = n_q // blocks
    flat = jnp.concatenate(
        [
            jnp.concatenate([o_s[2 * i], o_s[2 * i + 1]], axis=0).T.astype(BF16)
            for i in range(tiles)
        ],
        axis=0,
    )
    for b in range(blocks):
        out_ref[b, :rows] = flat[b * rows : (b + 1) * rows]
        for k in range(STAT_ROWS // 8):
            at = b * rows + k * LANES
            out_ref[b, rows + 8 * k : rows + 8 * k + 8] = stats[:, at : at + LANES].astype(BF16)


def combine_kernel(
    place_ref, part_ref, ga_ref, gated_b_ref, wa_ref, wb_ref, kept_ref, sent_ref, out_s
):
    blocks, padded, _ = part_ref.shape
    rows = padded - STAT_ROWS
    lses = []
    for s in range(blocks):
        pieces = [
            part_ref[s, rows + 8 * k : rows + 8 * k + 8].astype(F32) for k in range(STAT_ROWS // 8)
        ]
        x = jnp.concatenate(pieces, axis=1)
        lses.append(x[0:2] + x[2:4] + x[4:6])
    top = functools.reduce(jnp.maximum, lses)
    weights = [jnp.exp(v - top) for v in lses]
    den = functools.reduce(jnp.add, weights)
    stacked = jnp.concatenate([v / den for v in weights], axis=0)
    cols = jnp.concatenate(
        [stacked, jnp.zeros((LANES - 2 * blocks, stacked.shape[1]), F32)], axis=0
    ).T
    low = lax.broadcasted_iota(jnp.int32, (rows, LANES), 1) < HEAD
    acc = jnp.zeros((rows, LANES), F32)
    for s in range(blocks):
        w = jnp.where(low, cols[:rows, 2 * s : 2 * s + 1], cols[:rows, 2 * s + 1 : 2 * s + 2])
        acc = acc + w * part_ref[s, :rows].astype(F32)
    gated_a = (acc * silu(ga_ref[...].astype(F32))).astype(BF16)
    gated = jnp.concatenate([gated_a, gated_b_ref[...]], axis=1)
    w = jnp.concatenate([wa_ref[...], wb_ref[...]], axis=0)
    result = dot(gated, w).astype(BF16)
    core = place_ref[0]
    chips, piece, _ = kept_ref.shape
    for t in range(2 * chips):
        out_s[t] = result[t * piece : (t + 1) * piece]
    for i in range(chips):
        kept_ref[i] = out_s[2 * i + core]
        sent_ref[i] = out_s[2 * i + 1 - core]


def call(kernel, outs, scratch, smem, near, *args, name, flops=0, far=()):
    args = [
        pltpu.with_memory_space_constraint(a, pltpu.VMEM) if i in near else a
        for i, a in enumerate(args)
    ]
    specs = [
        pl.BlockSpec(
            memory_space=pltpu.SMEM if i in smem else pl.ANY if i in far else pltpu.VMEM
        )
        for i in range(len(args))
    ]
    return pl.pallas_call(
        kernel,
        out_shape=outs,
        in_specs=specs,
        out_specs=jax.tree.map(lambda _: pl.BlockSpec(memory_space=pltpu.VMEM), outs),
        scratch_shapes=scratch,
        compiler_params=pltpu.CompilerParams(vmem_limit_bytes=56 * 2**20),
        cost_estimate=pl.CostEstimate(flops=flops, bytes_accessed=2**20, transcendentals=0),
        name=name,
    )(*args)


def shaped(*shape, dtype=BF16):
    return jax.ShapeDtypeStruct(shape, dtype)


def body(
    tokens, norm_gain, w_qa, w_ka, w_va, qgain_a, kgain_a, w_qb, w_kb, w_vb, sink_b, w_ga, w_gb,
    out_a, out_b,
):
    rows, width = tokens.shape
    n_x = lax.axis_size("x")
    blocks = lax.axis_size(SP)
    n_y = lax.axis_size(Q_GROUP)
    n_z = lax.axis_size(K_GROUP)
    tp = 2 * n_x
    s_index = lax.axis_index(SP)
    core = lax.axis_index("core")
    place = jnp.stack([core, s_index]).astype(jnp.int32)
    row_table, col_table = rotary_tables(blocks * rows)

    mine = lax.all_gather(tokens, "x", axis=0)
    other = lax.ppermute(mine, "core", [(0, 1), (1, 0)])
    q, kv8, qb, kvb, kvb_first, kvb_last, ga, gb = call(
        project_kernel,
        (
            shaped(rows, LANES), shaped(n_z, rows, LANES),
            shaped(rows, LANES), shaped(rows, LANES),
            shaped(WINDOW, LANES), shaped(WINDOW, LANES),
            shaped(rows, LANES), shaped(rows, LANES),
        ),
        [
            pltpu.VMEM((tp, rows, width), BF16),
            pltpu.VMEM((4, tp * width, LANES), BF16),
            pltpu.VMEM((4 * HEAD, tp * width), BF16),
            pltpu.SemaphoreType.DMA((8,)),
        ],
        {0},
        {1, 2},
        place, mine, other, norm_gain.reshape(tp, 1, width), qgain_a, kgain_a,
        jnp.asarray(row_table), jnp.asarray(col_table),
        w_qa, w_ka.T, w_va.T, w_qb, w_kb.T, w_vb.T, w_ga, w_gb,
        name="project", flops=2 * rows * width * tp * 768, far=set(range(8, 16)),
    )
    kv_all = lax.all_to_all(kv8, K_GROUP, 0, 0, tiled=True)
    q_all = q
    for axis in reversed(Q_GROUP):
        q_all = lax.all_gather(q_all, axis, axis=0, tiled=True)
    up = [(i, i + 1) for i in range(blocks - 1)]
    down = [(i + 1, i) for i in range(blocks - 1)]
    before = lax.ppermute(kvb_last, SP, up)
    after = lax.ppermute(kvb_first, SP, down)
    q_all, before, after = lax.optimization_barrier((q_all, before, after))
    gated_b = call(
        functools.partial(window_kernel, count=blocks),
        shaped(rows, LANES),
        [],
        {0, 5},
        {3, 4},
        place, qb, kvb, before, after, sink_b, gb,
        name="windowed", flops=4 * 2 * rows * 576 * 64,
    )
    n_q = n_y * rows
    n_k = n_z * rows
    tile = 512
    chunk = 256
    steps = 2 * n_q // tile
    parts = call(
        functools.partial(attend_kernel, tile=tile, chunk=chunk),
        shaped(n_y, rows + STAT_ROWS, LANES),
        [
            pltpu.VMEM((n_k, LANES), BF16),
            pltpu.VMEM((n_k // chunk, ACC_ROWS, chunk), BF16),
            pltpu.VMEM((steps, LANES, tile), BF16),
            pltpu.VMEM((steps, 1, tile), F32),
            pltpu.VMEM((steps, HEAD, tile), F32),
            pltpu.VMEM((steps, 1, tile), F32),
            pltpu.VMEM((2, n_k // chunk, chunk, tile), BF16),
        ],
        {},
        {0, 1},
        q_all, kv_all.reshape(n_k, LANES),
        name="attend", flops=4 * 2 * n_q * n_k * 64,
    )
    back = lax.all_to_all(parts, Q_GROUP, 0, 0, tiled=True)
    piece = shaped(n_x, rows // tp, out_a.shape[1])
    kept, sent = call(
        combine_kernel,
        (piece, piece),
        [pltpu.VMEM((tp, rows // tp, out_a.shape[1]), BF16)],
        {0},
        {1, 4, 5},
        place, back, ga, gated_b, out_a, out_b,
        name="combine", flops=2 * rows * 256 * 2048,
    )
    got = lax.ppermute(sent, "core", [(0, 1), (1, 0)])
    paired = (kept.astype(F32) + got.astype(F32)).astype(BF16)
    arrived = lax.all_to_all(paired, "x", 0, 0, tiled=True)
    return jnp.sum(arrived.astype(F32), axis=0).astype(BF16)


def solution(mesh):
    n_tp = mesh.shape["tp"]
    fine = Mesh(np.asarray(mesh.devices).reshape(4, 2, 2, 4, n_tp // 2, 2), (*SP, *TP))
    sp = SP
    tp = TP
    placed = (
        P(sp, tp), P(), P(None, tp), P(None, tp), P(None, tp), P(tp, None), P(tp, None),
        P(None, tp), P(None, tp), P(None, tp), P(tp), P(None, tp), P(None, tp), P(tp, None),
        P(tp, None),
    )
    return jax.shard_map(
        body, mesh=fine, in_specs=placed, out_specs=P((*sp, *tp), None), check_vma=False
    )
```

```python
import functools

import jax
import jax.numpy as jnp
import numpy as np
from jax import lax
from jax.experimental import pallas as pl
from jax.experimental.pallas import tpu as pltpu
from jax.sharding import Mesh, PartitionSpec as P

GRID = 64
WINDOW = 128
EPSILON = 1e-06
THETA = 10000.0
HEAD = 64
LANES = 128
BOUND = 69.0
SHIFT = 55.0
STAT_ROWS = 24
F32 = jnp.float32
BF16 = jnp.bfloat16


def rotary_tables(seq):
    quarter = HEAD // 4
    freq = np.power(np.float32(THETA), -np.arange(quarter, dtype=np.float32) / np.float32(quarter))
    freq = freq.astype(np.float32)

    def table(count, which):
        angle = (np.arange(count, dtype=np.float32)[:, None] * freq).astype(np.float64)
        out = []
        for fn in (np.cos, np.sin):
            half = np.concatenate([fn(angle), fn(angle)], axis=1)
            zero = np.zeros_like(half)
            head = np.concatenate([half, zero] if which == 0 else [zero, half], axis=1)
            out.append(np.concatenate([head, head], axis=1).astype(np.float32))
        return np.stack(out)

    return table(seq // GRID, 0), table(GRID, 1)


def dot(a, b):
    return jnp.dot(a, b, preferred_element_type=F32)


def dot_t(a, b):
    return lax.dot_general(a, b, (((1,), (1,)), ((), ())), preferred_element_type=F32)


def silu(v):
    return v / (1.0 + jnp.exp(-v))


def project_kernel(
    place_ref, mine_ref, other_ref, gain_ref, qgain_ref, kgain_ref, row_ref, col_ref,
    wqa, wka, wva, wqb, wkb, wvb, wga, wgb,
    q_out, kv_out, qb_out, kvb_out, first_out, last_out, ga_out, gb_out,
    h_s, wide_s, narrow_s, sems,
):
    wide = [wqa, wqb, wga, wgb]
    narrow = [wka, wva, wkb, wvb]
    copies = [
        pltpu.make_async_copy(ref, narrow_s.at[i * HEAD : (i + 1) * HEAD], sems.at[i])
        for i, ref in enumerate(narrow)
    ]
    copies += [
        pltpu.make_async_copy(ref, wide_s.at[i], sems.at[4 + i]) for i, ref in enumerate(wide)
    ]
    for copy in copies:
        copy.start()
    core = place_ref[0]
    s_index = place_ref[1]
    chips, rows, width = mine_ref.shape
    total = jnp.zeros((rows, 1), F32)
    for ref in (mine_ref, other_ref):
        for i in range(chips):
            part = ref[i].astype(F32)
            total = total + jnp.sum(part * part, axis=1, keepdims=True)
    scale = lax.rsqrt(total / (2 * chips * width) + EPSILON)
    for ref, side in ((mine_ref, core), (other_ref, 1 - core)):
        for i in range(chips):
            t = 2 * i + side
            h_s[t] = (ref[i].astype(F32) * scale * gain_ref[t]).astype(BF16)
    normed = jnp.concatenate([h_s[t] for t in range(2 * chips)], axis=1)
    for copy in copies:
        copy.wait()
    both_kv = dot_t(normed, narrow_s[...])
    both_q = dot(normed, jnp.concatenate([wide_s[0], wide_s[1]], axis=1))
    both_g = dot(normed, jnp.concatenate([wide_s[2], wide_s[3]], axis=1))
    ga_out[...] = both_g[:, :LANES].astype(BF16)
    gb_out[...] = both_g[:, LANES:].astype(BF16)
    qb_out[...] = both_q[:, LANES:].astype(BF16)
    kvb = both_kv[:, LANES:].astype(BF16)
    kvb_out[...] = kvb
    first_out[...] = kvb[:WINDOW]
    last_out[...] = kvb[rows - WINDOW :]
    cos = []
    sin = []
    grid_rows = rows // GRID
    for r in range(grid_rows):
        at = s_index * grid_rows + r
        cos.append(row_ref[0, pl.ds(at, 1), :] + col_ref[0])
        sin.append(row_ref[1, pl.ds(at, 1), :] + col_ref[1])
    cos = jnp.concatenate(cos, axis=0)
    sin = jnp.concatenate(sin, axis=0)
    lane = lax.broadcasted_iota(jnp.int32, (rows, LANES), 1)
    first = (lane % 32) < 16
    low = lane < HEAD

    def turned(n):
        partner = jnp.where(first, -pltpu.roll(n, LANES - 16, 1), pltpu.roll(n, 16, 1))
        return n * cos + partner * sin

    v = both_q[:, :LANES].astype(BF16).astype(F32)
    square = v * v
    sum_low = jnp.sum(jnp.where(low, square, 0.0), axis=1, keepdims=True)
    sum_high = jnp.sum(jnp.where(low, 0.0, square), axis=1, keepdims=True)
    rs_low = lax.rsqrt(sum_low / HEAD + EPSILON)
    rs_high = lax.rsqrt(sum_high / HEAD + EPSILON)
    qgain = jnp.concatenate([qgain_ref[0:1, :], qgain_ref[1:2, :]], axis=1)
    q_out[...] = turned(v * jnp.where(low, rs_low, rs_high) * qgain).astype(BF16)
    kv = both_kv[:, :LANES].astype(BF16).astype(F32)
    k_only = jnp.where(low, kv, 0.0)
    sq = jnp.sum(k_only * k_only, axis=1, keepdims=True)
    kgain = jnp.concatenate([kgain_ref[...], kgain_ref[...]], axis=1)
    ka = turned(k_only * lax.rsqrt(sq / HEAD + EPSILON) * kgain)
    both = jnp.where(low, ka, kv).astype(BF16)
    for i in range(kv_out.shape[0]):
        kv_out[i] = both


def window_kernel(
    place_ref, q_ref, mid_ref, prev_ref, next_ref, sink_ref, gate_ref, out_ref, *, count
):
    s_index = place_ref[1]
    rows = q_ref.shape[0]
    kv = jnp.concatenate([prev_ref[...], mid_ref[...], next_ref[...]], axis=0)
    span = kv.shape[0]
    r = lax.broadcasted_iota(jnp.int32, (rows, span), 0)
    c = lax.broadcasted_iota(jnp.int32, (rows, span), 1)
    place = s_index * rows - WINDOW + c
    allowed = (c >= r) & (c - r <= 2 * WINDOW) & (place >= 0) & (place < rows * count)
    q = q_ref[...] * HEAD ** (-0.5)
    stacked = jnp.concatenate([q[:, :HEAD], q[:, HEAD:]], axis=0)
    scores = dot_t(stacked, kv[:, :HEAD])
    terms = []
    dens = []
    for h in range(2):
        s = jnp.where(allowed, scores[h * rows : (h + 1) * rows], -1e30)
        sink = sink_ref[h]
        top = jnp.maximum(jnp.max(s, axis=1, keepdims=True), sink)
        p = jnp.exp(s - top)
        dens.append(jnp.sum(p, axis=1, keepdims=True) + jnp.exp(sink - top))
        terms.append(p.astype(BF16))
    mixed = dot(jnp.concatenate(terms, axis=0), kv[:, HEAD:])
    att = jnp.concatenate([mixed[:rows] / dens[0], mixed[rows:] / dens[1]], axis=1)
    out_ref[...] = (att * silu(gate_ref[...].astype(F32))).astype(BF16)


def attend_kernel(
    q_ref, kv_ref, out_ref, k_s, vt_s, qt_s, m_s, o_s, lse_s, p_s, l_s, *, tile, chunk
):
    n_q = q_ref.shape[0]
    n_k = kv_ref.shape[0]
    tiles = n_q // tile
    steps = 2 * tiles
    chunks = n_k // chunk
    kv = kv_ref[...]
    lane = lax.broadcasted_iota(jnp.int32, (n_k, LANES), 1)
    ones = jnp.where(lane < HEAD + 3, 1.0, 0.0)
    k_s[...] = jnp.where(lane < HEAD, kv.astype(F32), ones).astype(BF16)
    kv_t = kv.astype(F32).T
    k_t = kv_t[:HEAD]
    k_norm = jnp.max(jnp.sum(k_t * k_t, axis=0, keepdims=True))
    for c in range(chunks):
        vt_s[c] = kv_t[HEAD:, c * chunk : (c + 1) * chunk].astype(BF16)
    top = jnp.float32(0.0)
    for i in range(tiles):
        q_t = q_ref[i * tile : (i + 1) * tile, :].astype(F32).T
        for h in range(2):
            part = q_t[h * HEAD : (h + 1) * HEAD] * HEAD ** (-0.5)
            bound = jnp.sqrt(jnp.sum(part * part, axis=0, keepdims=True) * k_norm) * 1.0001
            top = jnp.maximum(top, jnp.max(bound))
            m_s[2 * i + h] = bound - SHIFT
            qt_s[2 * i + h, :HEAD] = part.astype(BF16)
            qt_s[2 * i + h, HEAD:] = jnp.zeros((LANES - HEAD, tile), BF16)

    @pl.when(top > BOUND)
    def _():
        def row_max(t, carry):
            def one(c, m):
                s = dot(k_s[pl.ds(pl.multiple_of(c * chunk, chunk), chunk), :], qt_s[t])
                return jnp.maximum(m, jnp.max(s, axis=0, keepdims=True))

            m_s[t] = lax.fori_loop(0, chunks, one, jnp.full((1, tile), -1e30, F32))
            return carry

        lax.fori_loop(0, steps, row_max, 0)

    row = lax.broadcasted_iota(jnp.int32, (16, tile), 0)
    for t in range(steps):
        neg = -m_s[t]
        hi = neg.astype(BF16).astype(F32)
        mid = (neg - hi).astype(BF16).astype(F32)
        lo = neg - hi - mid
        parts = jnp.where(row == 0, hi, jnp.where(row == 1, mid, jnp.where(row == 2, lo, 0.0)))
        qt_s[t, HEAD : HEAD + 16] = parts.astype(BF16)

    def both(ahead, ahead_slot, now, now_slot):
        if ahead is not None:
            q_here = qt_s[ahead]
            sums = jnp.zeros((8, tile), F32)
        acc = jnp.zeros((HEAD, tile), F32)
        for c in range(chunks):
            if ahead is not None:
                e = jnp.exp(dot(k_s[c * chunk : (c + 1) * chunk, :], q_here))
                sums = sums + jnp.sum(e.reshape(chunk // 8, 8, tile), axis=0)
                p_s[ahead_slot, c] = e.astype(BF16)
            if now is not None:
                acc = acc + dot(vt_s[c], p_s[now_slot, c])
        if now is not None:
            total = jnp.sum(l_s[now_slot], axis=0, keepdims=True)
            lse_s[now] = m_s[now] + jnp.log(total)
            o_s[now] = acc / total
        if ahead is not None:
            l_s[ahead_slot] = sums

    both(0, 0, None, None)

    def pair(n, carry):
        both(2 * n + 1, 1, 2 * n, 0)
        both(2 * n + 2, 0, 2 * n + 1, 1)
        return carry

    lax.fori_loop(0, (steps - 2) // 2, pair, 0)
    both(steps - 1, 1, steps - 2, 0)
    both(None, None, steps - 1, 1)

    lse = jnp.concatenate(
        [jnp.concatenate([lse_s[2 * i], lse_s[2 * i + 1]], axis=0) for i in range(tiles)], axis=1
    )
    hi = lse.astype(BF16).astype(F32)
    mid = (lse - hi).astype(BF16).astype(F32)
    lo = lse - hi - mid
    stats = jnp.concatenate([hi, mid, lo, jnp.zeros_like(hi)], axis=0)
    stats = jnp.concatenate([stats, jnp.zeros((8, LANES), F32)], axis=1)
    blocks = out_ref.shape[0]
    rows = n_q // blocks
    flat = jnp.concatenate(
        [
            jnp.concatenate([o_s[2 * i], o_s[2 * i + 1]], axis=0).T.astype(BF16)
            for i in range(tiles)
        ],
        axis=0,
    )
    for b in range(blocks):
        out_ref[b, :rows] = flat[b * rows : (b + 1) * rows]
        for k in range(STAT_ROWS // 8):
            at = b * rows + k * LANES
            out_ref[b, rows + 8 * k : rows + 8 * k + 8] = stats[:, at : at + LANES].astype(BF16)


def combine_kernel(
    place_ref, part_ref, ga_ref, gated_b_ref, wa_ref, wb_ref, kept_ref, sent_ref, out_s
):
    blocks, padded, _ = part_ref.shape
    rows = padded - STAT_ROWS
    lses = []
    for s in range(blocks):
        pieces = [
            part_ref[s, rows + 8 * k : rows + 8 * k + 8].astype(F32) for k in range(STAT_ROWS // 8)
        ]
        x = jnp.concatenate(pieces, axis=1)
        lses.append(x[0:2] + x[2:4] + x[4:6])
    top = functools.reduce(jnp.maximum, lses)
    weights = [jnp.exp(v - top) for v in lses]
    den = functools.reduce(jnp.add, weights)
    stacked = jnp.concatenate([v / den for v in weights], axis=0)
    cols = jnp.concatenate(
        [stacked, jnp.zeros((LANES - 2 * blocks, stacked.shape[1]), F32)], axis=0
    ).T
    low = lax.broadcasted_iota(jnp.int32, (rows, LANES), 1) < HEAD
    acc = jnp.zeros((rows, LANES), F32)
    for s in range(blocks):
        w = jnp.where(low, cols[:rows, 2 * s : 2 * s + 1], cols[:rows, 2 * s + 1 : 2 * s + 2])
        acc = acc + w * part_ref[s, :rows].astype(F32)
    gated_a = (acc * silu(ga_ref[...].astype(F32))).astype(BF16)
    gated = jnp.concatenate([gated_a, gated_b_ref[...]], axis=1)
    w = jnp.concatenate([wa_ref[...], wb_ref[...]], axis=0)
    result = dot(gated, w).astype(BF16)
    core = place_ref[0]
    chips, piece, _ = kept_ref.shape
    for t in range(2 * chips):
        out_s[t] = result[t * piece : (t + 1) * piece]
    for i in range(chips):
        kept_ref[i] = out_s[2 * i + core]
        sent_ref[i] = out_s[2 * i + 1 - core]


def call(kernel, outs, scratch, smem, near, *args, name, flops=0, far=()):
    args = [
        pltpu.with_memory_space_constraint(a, pltpu.VMEM) if i in near else a
        for i, a in enumerate(args)
    ]
    specs = [
        pl.BlockSpec(
            memory_space=pltpu.SMEM if i in smem else pl.ANY if i in far else pltpu.VMEM
        )
        for i in range(len(args))
    ]
    return pl.pallas_call(
        kernel,
        out_shape=outs,
        in_specs=specs,
        out_specs=(
            tuple(pl.BlockSpec(memory_space=pltpu.VMEM) for _ in outs)
            if isinstance(outs, tuple)
            else pl.BlockSpec(memory_space=pltpu.VMEM)
        ),
        scratch_shapes=scratch,
        compiler_params=pltpu.CompilerParams(vmem_limit_bytes=56 * 2**20),
        cost_estimate=pl.CostEstimate(flops=flops, bytes_accessed=2**20, transcendentals=0),
        name=name,
    )(*args)


def shaped(*shape, dtype=BF16):
    return pltpu.VMEM(shape, dtype)


def body(
    tokens, norm_gain, w_qa, w_ka, w_va, qgain_a, kgain_a, w_qb, w_kb, w_vb, sink_b, w_ga, w_gb,
    out_a, out_b,
):
    rows, width = tokens.shape
    n_z, n_y, n_x = (lax.axis_size(a) for a in ("z", "y", "x"))
    blocks = n_z * n_y
    tp = 2 * n_x
    s_index = lax.axis_index("z") * n_y + lax.axis_index("y")
    core = lax.axis_index("core")
    place = jnp.stack([core, s_index]).astype(jnp.int32)
    row_table, col_table = rotary_tables(blocks * rows)

    mine = lax.all_gather(tokens, "x", axis=0)
    other = lax.ppermute(mine, "core", [(0, 1), (1, 0)])
    q, kv8, qb, kvb, kvb_first, kvb_last, ga, gb = call(
        project_kernel,
        (
            shaped(rows, LANES), shaped(n_z, rows, LANES),
            shaped(rows, LANES), shaped(rows, LANES),
            shaped(WINDOW, LANES), shaped(WINDOW, LANES),
            shaped(rows, LANES), shaped(rows, LANES),
        ),
        [
            pltpu.VMEM((tp, rows, width), BF16),
            pltpu.VMEM((4, tp * width, LANES), BF16),
            pltpu.VMEM((4 * HEAD, tp * width), BF16),
            pltpu.SemaphoreType.DMA((8,)),
        ],
        {0},
        {1, 2},
        place, mine, other, norm_gain.reshape(tp, 1, width), qgain_a, kgain_a,
        jnp.asarray(row_table), jnp.asarray(col_table),
        w_qa, w_ka.T, w_va.T, w_qb, w_kb.T, w_vb.T, w_ga, w_gb,
        name="project", flops=2 * rows * width * tp * 768, far=set(range(8, 16)),
    )
    kv_all = lax.all_to_all(kv8, "z", 0, 0, tiled=True)
    q_all = lax.all_gather(q, "y", axis=0, tiled=True)
    up = [(i, i + 1) for i in range(blocks - 1)]
    down = [(i + 1, i) for i in range(blocks - 1)]
    before = lax.ppermute(kvb_last, ("z", "y"), up)
    after = lax.ppermute(kvb_first, ("z", "y"), down)
    gated_b = call(
        functools.partial(window_kernel, count=blocks),
        shaped(rows, LANES),
        [],
        {0, 5},
        {1, 2, 3, 4, 6},
        place, qb, kvb, before, after, sink_b, gb,
        name="windowed", flops=4 * 2 * rows * 576 * 64,
    )
    n_q = n_y * rows
    n_k = n_z * rows
    tile = 512
    chunk = 256
    steps = 2 * n_q // tile
    parts = call(
        functools.partial(attend_kernel, tile=tile, chunk=chunk),
        shaped(n_y, rows + STAT_ROWS, LANES),
        [
            pltpu.VMEM((n_k, LANES), BF16),
            pltpu.VMEM((n_k // chunk, HEAD, chunk), BF16),
            pltpu.VMEM((steps, LANES, tile), BF16),
            pltpu.VMEM((steps, 1, tile), F32),
            pltpu.VMEM((steps, HEAD, tile), F32),
            pltpu.VMEM((steps, 1, tile), F32),
            pltpu.VMEM((2, n_k // chunk, chunk, tile), BF16),
            pltpu.VMEM((2, 8, tile), F32),
        ],
        {},
        {0, 1},
        q_all, kv_all.reshape(n_k, LANES),
        name="attend", flops=4 * 2 * n_q * n_k * 64,
    )
    back = lax.all_to_all(parts, "y", 0, 0, tiled=True)
    piece = shaped(n_x, rows // tp, out_a.shape[1])
    kept, sent = call(
        combine_kernel,
        (piece, piece),
        [pltpu.VMEM((tp, rows // tp, out_a.shape[1]), BF16)],
        {0},
        {1, 2, 3, 4, 5},
        place, back, ga, gated_b, out_a, out_b,
        name="combine", flops=2 * rows * 256 * 2048,
    )
    got = lax.ppermute(sent, "core", [(0, 1), (1, 0)])
    paired = (kept.astype(F32) + got.astype(F32)).astype(BF16)
    arrived = lax.all_to_all(paired, "x", 0, 0, tiled=True)
    return jnp.sum(arrived.astype(F32), axis=0).astype(BF16)


def solution(mesh):
    n_sp, n_tp = (mesh.shape["sp"], mesh.shape["tp"])
    n_z = 8
    fine = Mesh(
        np.asarray(mesh.devices).reshape(n_z, n_sp // n_z, n_tp // 2, 2), ("z", "y", "x", "core")
    )
    sp = ("z", "y")
    tp = ("x", "core")
    placed = (
        P(sp, tp), P(), P(None, tp), P(None, tp), P(None, tp), P(tp, None), P(tp, None),
        P(None, tp), P(None, tp), P(None, tp), P(tp), P(None, tp), P(None, tp), P(tp, None),
        P(tp, None),
    )
    return jax.shard_map(
        body, mesh=fine, in_specs=placed, out_specs=P((*sp, *tp), None), check_vma=False
    )
```

```python
import functools

import jax
import jax.numpy as jnp
import numpy as np
from jax import lax
from jax.experimental import pallas as pl
from jax.experimental.pallas import tpu as pltpu
from jax.sharding import Mesh, PartitionSpec as P

GRID = 64
WINDOW = 128
EPSILON = 1e-06
THETA = 10000.0
HEAD = 64
LANES = 128
BOUND = 69.0
SHIFT = 55.0
STAT_ROWS = 24
F32 = jnp.float32
BF16 = jnp.bfloat16


def rotary_tables(seq, blocks):
    quarter = HEAD // 4
    freq = np.power(np.float32(THETA), -np.arange(quarter, dtype=np.float32) / np.float32(quarter))
    freq = freq.astype(np.float32)

    def table(count, which):
        angle = (np.arange(count, dtype=np.float32)[:, None] * freq).astype(np.float64)
        out = []
        for fn in (np.cos, np.sin):
            half = np.concatenate([fn(angle), fn(angle)], axis=1)
            zero = np.zeros_like(half)
            head = np.concatenate([half, zero] if which == 0 else [zero, half], axis=1)
            out.append(np.concatenate([head, head], axis=1).astype(np.float32))
        return np.stack(out)

    by_row = table(seq // GRID, 0).reshape(2, blocks, -1, LANES)
    padded = np.zeros((blocks, 16, LANES), np.float32)
    padded[:, : by_row.shape[2]] = by_row[0]
    padded[:, 8 : 8 + by_row.shape[2]] = by_row[1]
    return padded, table(GRID, 1)


def dot(a, b):
    return jnp.dot(a, b, preferred_element_type=F32)


def dot_t(a, b):
    return lax.dot_general(a, b, (((1,), (1,)), ((), ())), preferred_element_type=F32)


def silu(v):
    return v / (1.0 + jnp.exp(-v))


def project_kernel(
    place_ref, mine_ref, other_ref, gain_ref, qgain_ref, kgain_ref, col_ref, row_ref,
    wqa, wka, wva, wqb, wkb, wvb,
    q_out, kv_out, qb_out, kvb_out, first_out, last_out, h_out,
    h_s, wide_s, narrow_s, row_s, sems,
):
    core = place_ref[0]
    wide = [wqa, wqb]
    narrow = [wka, wva, wkb, wvb]
    copies = [pltpu.make_async_copy(row_ref.at[place_ref[1]], row_s, sems.at[6])]
    copies += [
        pltpu.make_async_copy(ref, narrow_s.at[i * HEAD : (i + 1) * HEAD], sems.at[i])
        for i, ref in enumerate(narrow)
    ]
    copies += [
        pltpu.make_async_copy(ref, wide_s.at[i], sems.at[4 + i]) for i, ref in enumerate(wide)
    ]
    for copy in copies:
        copy.start()
    chips, rows, width = mine_ref.shape
    count = 2 * chips
    block = GRID

    def normalise(r, carry):
        at = pl.ds(pl.multiple_of(r * block, block), block)
        parts = [ref[i, at, :].astype(F32) for ref in (mine_ref, other_ref) for i in range(chips)]
        squares = functools.reduce(jnp.add, [v * v for v in parts])
        total = jnp.sum(squares, axis=1, keepdims=True)
        scale = lax.rsqrt(total / (count * width) + EPSILON)
        for n, v in enumerate(parts):
            t = 2 * (n % chips) + (core if n < chips else 1 - core)
            h_s[t, at, :] = (v * scale * gain_ref[t]).astype(BF16)
        return carry

    lax.fori_loop(0, rows // block, normalise, 0)
    normed = jnp.concatenate([h_s[t] for t in range(count)], axis=1)
    h_out[...] = normed
    for copy in copies:
        copy.wait()
    both_kv = dot_t(normed, narrow_s[...])
    both_q = dot(normed, jnp.concatenate([wide_s[0], wide_s[1]], axis=1))
    qb_out[...] = both_q[:, LANES:].astype(BF16)
    kvb = both_kv[:, LANES:].astype(BF16)
    kvb_out[...] = kvb
    first_out[...] = kvb[:WINDOW]
    last_out[...] = kvb[rows - WINDOW :]
    grid_rows = rows // GRID
    cos = jnp.concatenate([row_s[r : r + 1] + col_ref[0] for r in range(grid_rows)], axis=0)
    sin = jnp.concatenate([row_s[8 + r : 9 + r] + col_ref[1] for r in range(grid_rows)], axis=0)
    lane = lax.broadcasted_iota(jnp.int32, (rows, LANES), 1)
    first = (lane % 32) < 16
    low = lane < HEAD

    def turned(n):
        partner = jnp.where(first, -pltpu.roll(n, LANES - 16, 1), pltpu.roll(n, 16, 1))
        return n * cos + partner * sin

    v = both_q[:, :LANES].astype(BF16).astype(F32)
    square = v * v
    sum_low = jnp.sum(jnp.where(low, square, 0.0), axis=1, keepdims=True)
    sum_high = jnp.sum(jnp.where(low, 0.0, square), axis=1, keepdims=True)
    rs_low = lax.rsqrt(sum_low / HEAD + EPSILON)
    rs_high = lax.rsqrt(sum_high / HEAD + EPSILON)
    qgain = jnp.concatenate([qgain_ref[0:1, :], qgain_ref[1:2, :]], axis=1)
    qa = turned(v * jnp.where(low, rs_low, rs_high) * qgain).astype(BF16)
    for i in range(q_out.shape[0]):
        q_out[i] = qa
    kv = both_kv[:, :LANES].astype(BF16).astype(F32)
    k_only = jnp.where(low, kv, 0.0)
    sq = jnp.sum(k_only * k_only, axis=1, keepdims=True)
    kgain = jnp.concatenate([kgain_ref[...], kgain_ref[...]], axis=1)
    ka = turned(k_only * lax.rsqrt(sq / HEAD + EPSILON) * kgain)
    kv_out[...] = jnp.where(low, ka, kv).astype(BF16)


def gate_kernel(h_ref, wa_ref, wb_ref, ga_out, gb_out):
    both = dot(h_ref[...], jnp.concatenate([wa_ref[...], wb_ref[...]], axis=1))
    gates = silu(both.astype(BF16).astype(F32))
    ga_out[...] = gates[:, :LANES]
    gb_out[...] = gates[:, LANES:]


def window_kernel(
    place_ref, q_ref, mid_ref, prev_ref, next_ref, sink_ref, gate_ref, out_ref, *, count
):
    s_index = place_ref[1]
    rows = q_ref.shape[0]
    kv = jnp.concatenate([prev_ref[...], mid_ref[...], next_ref[...]], axis=0)
    span = kv.shape[0]
    r = lax.broadcasted_iota(jnp.int32, (rows, span), 0)
    c = lax.broadcasted_iota(jnp.int32, (rows, span), 1)
    place = s_index * rows - WINDOW + c
    allowed = (c >= r) & (c - r <= 2 * WINDOW) & (place >= 0) & (place < rows * count)
    q = q_ref[...] * HEAD ** (-0.5)
    stacked = jnp.concatenate([q[:, :HEAD], q[:, HEAD:]], axis=0)
    scores = dot_t(stacked, kv[:, :HEAD])
    terms = []
    dens = []
    for h in range(2):
        s = jnp.where(allowed, scores[h * rows : (h + 1) * rows], -1e30)
        sink = sink_ref[h]
        top = jnp.maximum(jnp.max(s, axis=1, keepdims=True), sink)
        p = jnp.exp(s - top)
        dens.append(jnp.sum(p, axis=1, keepdims=True) + jnp.exp(sink - top))
        terms.append(p.astype(BF16))
    mixed = dot(jnp.concatenate(terms, axis=0), kv[:, HEAD:])
    att = jnp.concatenate([mixed[:rows] / dens[0], mixed[rows:] / dens[1]], axis=1)
    out_ref[...] = (att * gate_ref[...]).astype(BF16)


def attend_kernel(
    q_ref, kv_ref, out_ref, k_s, vt_s, qt_s, m_s, o_s, lse_s, p_s, l_s, *, tile, chunk
):
    n_q = q_ref.shape[0]
    n_k = kv_ref.shape[0]
    tiles = n_q // tile
    steps = 2 * tiles
    chunks = n_k // chunk
    kv = kv_ref[...]
    lane = lax.broadcasted_iota(jnp.int32, (n_k, LANES), 1)
    ones = jnp.where(lane < HEAD + 3, 1.0, 0.0)
    k_s[...] = jnp.where(lane < HEAD, kv.astype(F32), ones).astype(BF16)
    kv_t = kv.astype(F32).T
    k_t = kv_t[:HEAD]
    k_norm = jnp.max(jnp.sum(k_t * k_t, axis=0, keepdims=True))
    for c in range(chunks):
        vt_s[c] = kv_t[HEAD:, c * chunk : (c + 1) * chunk].astype(BF16)
    top = jnp.float32(0.0)
    for i in range(tiles):
        q_t = q_ref[i * tile : (i + 1) * tile, :].astype(F32).T
        for h in range(2):
            part = q_t[h * HEAD : (h + 1) * HEAD] * HEAD ** (-0.5)
            bound = jnp.sqrt(jnp.sum(part * part, axis=0, keepdims=True) * k_norm) * 1.0001
            top = jnp.maximum(top, jnp.max(bound))
            m_s[2 * i + h] = bound - SHIFT
            qt_s[2 * i + h, :HEAD] = part.astype(BF16)
            qt_s[2 * i + h, HEAD:] = jnp.zeros((LANES - HEAD, tile), BF16)

    @pl.when(top > BOUND)
    def _():
        def row_max(t, carry):
            def one(c, m):
                s = dot(k_s[pl.ds(pl.multiple_of(c * chunk, chunk), chunk), :], qt_s[t])
                return jnp.maximum(m, jnp.max(s, axis=0, keepdims=True))

            m_s[t] = lax.fori_loop(0, chunks, one, jnp.full((1, tile), -1e30, F32))
            return carry

        lax.fori_loop(0, steps, row_max, 0)

    row = lax.broadcasted_iota(jnp.int32, (16, tile), 0)
    for t in range(steps):
        neg = -m_s[t]
        hi = neg.astype(BF16).astype(F32)
        mid = (neg - hi).astype(BF16).astype(F32)
        lo = neg - hi - mid
        parts = jnp.where(row == 0, hi, jnp.where(row == 1, mid, jnp.where(row == 2, lo, 0.0)))
        qt_s[t, HEAD : HEAD + 16] = parts.astype(BF16)

    def both(ahead, ahead_slot, now, now_slot):
        if ahead is not None:
            q_here = qt_s[ahead]
            sums = jnp.zeros((8, tile), F32)
        acc = jnp.zeros((HEAD, tile), F32)
        for c in range(chunks):
            if ahead is not None:
                e = jnp.exp(dot(k_s[c * chunk : (c + 1) * chunk, :], q_here))
                sums = sums + jnp.sum(e.reshape(chunk // 8, 8, tile), axis=0)
                p_s[ahead_slot, c] = e.astype(BF16)
            if now is not None:
                acc = acc + dot(vt_s[c], p_s[now_slot, c])
        if now is not None:
            total = jnp.sum(l_s[now_slot], axis=0, keepdims=True)
            lse_s[now] = m_s[now] + jnp.log(total)
            o_s[now] = acc / total
        if ahead is not None:
            l_s[ahead_slot] = sums

    both(0, 0, None, None)

    def pair(n, carry):
        both(2 * n + 1, 1, 2 * n, 0)
        both(2 * n + 2, 0, 2 * n + 1, 1)
        return carry

    lax.fori_loop(0, (steps - 2) // 2, pair, 0)
    both(steps - 1, 1, steps - 2, 0)
    both(None, None, steps - 1, 1)

    lse = jnp.concatenate(
        [jnp.concatenate([lse_s[2 * i], lse_s[2 * i + 1]], axis=0) for i in range(tiles)], axis=1
    )
    hi = lse.astype(BF16).astype(F32)
    mid = (lse - hi).astype(BF16).astype(F32)
    lo = lse - hi - mid
    stats = jnp.concatenate([hi, mid, lo, jnp.zeros_like(hi)], axis=0)
    stats = jnp.concatenate([stats, jnp.zeros((8, LANES), F32)], axis=1)
    blocks = out_ref.shape[0]
    rows = n_q // blocks
    flat = jnp.concatenate(
        [
            jnp.concatenate([o_s[2 * i], o_s[2 * i + 1]], axis=0).T.astype(BF16)
            for i in range(tiles)
        ],
        axis=0,
    )
    for b in range(blocks):
        out_ref[b, :rows] = flat[b * rows : (b + 1) * rows]
        for k in range(STAT_ROWS // 8):
            at = b * rows + k * LANES
            out_ref[b, rows + 8 * k : rows + 8 * k + 8] = stats[:, at : at + LANES].astype(BF16)


def combine_kernel(
    place_ref, part_ref, ga_ref, gated_b_ref, wa_ref, wb_ref, kept_ref, sent_ref, out_s
):
    blocks, padded, _ = part_ref.shape
    rows = padded - STAT_ROWS
    lses = []
    for s in range(blocks):
        pieces = [
            part_ref[s, rows + 8 * k : rows + 8 * k + 8].astype(F32) for k in range(STAT_ROWS // 8)
        ]
        x = jnp.concatenate(pieces, axis=1)
        lses.append(x[0:2] + x[2:4] + x[4:6])
    top = functools.reduce(jnp.maximum, lses)
    weights = [jnp.exp(v - top) for v in lses]
    den = functools.reduce(jnp.add, weights)
    stacked = jnp.concatenate([v / den for v in weights], axis=0)
    cols = jnp.concatenate(
        [stacked, jnp.zeros((LANES - 2 * blocks, stacked.shape[1]), F32)], axis=0
    ).T
    low = lax.broadcasted_iota(jnp.int32, (rows, LANES), 1) < HEAD
    acc = jnp.zeros((rows, LANES), F32)
    for s in range(blocks):
        w = jnp.where(low, cols[:rows, 2 * s : 2 * s + 1], cols[:rows, 2 * s + 1 : 2 * s + 2])
        acc = acc + w * part_ref[s, :rows].astype(F32)
    gated_a = (acc * ga_ref[...]).astype(BF16)
    gated = jnp.concatenate([gated_a, gated_b_ref[...]], axis=1)
    w = jnp.concatenate([wa_ref[...], wb_ref[...]], axis=0)
    result = dot(gated, w).astype(BF16)
    core = place_ref[0]
    chips, piece, _ = kept_ref.shape
    for t in range(2 * chips):
        out_s[t] = result[t * piece : (t + 1) * piece]
    for i in range(chips):
        kept_ref[i] = out_s[2 * i + core]
        sent_ref[i] = out_s[2 * i + 1 - core]


def call(kernel, outs, scratch, smem, near, *args, name, flops=0, far=()):
    args = [
        pltpu.with_memory_space_constraint(a, pltpu.VMEM) if i in near else a
        for i, a in enumerate(args)
    ]
    specs = [
        pl.BlockSpec(
            memory_space=pltpu.SMEM if i in smem else pl.ANY if i in far else pltpu.VMEM
        )
        for i in range(len(args))
    ]
    return pl.pallas_call(
        kernel,
        out_shape=outs,
        in_specs=specs,
        out_specs=(
            tuple(pl.BlockSpec(memory_space=pltpu.VMEM) for _ in outs)
            if isinstance(outs, tuple)
            else pl.BlockSpec(memory_space=pltpu.VMEM)
        ),
        scratch_shapes=scratch,
        compiler_params=pltpu.CompilerParams(vmem_limit_bytes=56 * 2**20),
        cost_estimate=pl.CostEstimate(flops=flops, bytes_accessed=2**20, transcendentals=0),
        name=name,
    )(*args)


def shaped(*shape, dtype=BF16):
    return pltpu.VMEM(shape, dtype)


def body(
    tokens, norm_gain, w_qa, w_ka, w_va, qgain_a, kgain_a, w_qb, w_kb, w_vb, sink_b, w_ga, w_gb,
    out_a, out_b,
):
    rows, width = tokens.shape
    n_z, n_y, n_x = (lax.axis_size(a) for a in ("z", "y", "x"))
    blocks = n_z * n_y
    tp = 2 * n_x
    s_index = lax.axis_index("z") * n_y + lax.axis_index("y")
    core = lax.axis_index("core")
    place = jnp.stack([core, s_index]).astype(jnp.int32)
    row_table, col_table = rotary_tables(blocks * rows, blocks)

    mine = lax.all_gather(tokens, "x", axis=0)
    other = lax.ppermute(mine, "core", [(0, 1), (1, 0)])
    q8, kv, qb, kvb, kvb_first, kvb_last, normed = call(
        project_kernel,
        (
            shaped(n_z, rows, LANES), shaped(rows, LANES),
            shaped(rows, LANES), shaped(rows, LANES),
            shaped(WINDOW, LANES), shaped(WINDOW, LANES),
            shaped(rows, tp * width),
        ),
        [
            pltpu.VMEM((tp, rows, width), BF16),
            pltpu.VMEM((2, tp * width, LANES), BF16),
            pltpu.VMEM((4 * HEAD, tp * width), BF16),
            pltpu.VMEM((16, LANES), F32),
            pltpu.SemaphoreType.DMA((7,)),
        ],
        {0},
        {1, 2},
        place, mine, other, norm_gain.reshape(tp, 1, width), qgain_a, kgain_a,
        jnp.asarray(col_table), jnp.asarray(row_table),
        w_qa, w_ka.T, w_va.T, w_qb, w_kb.T, w_vb.T,
        name="project", flops=2 * rows * width * tp * 512, far=set(range(7, 14)),
    )
    q_all = lax.all_to_all(q8, "z", 0, 0, tiled=True)
    kv_all = lax.all_gather(kv, "y", axis=0, tiled=True)
    up = [(i, i + 1) for i in range(blocks - 1)]
    down = [(i + 1, i) for i in range(blocks - 1)]
    before = lax.ppermute(kvb_last, ("z", "y"), up)
    after = lax.ppermute(kvb_first, ("z", "y"), down)
    n_q = n_z * rows
    n_k = n_y * rows
    tile = 512
    chunk = 256
    steps = 2 * n_q // tile
    parts = call(
        functools.partial(attend_kernel, tile=tile, chunk=chunk),
        shaped(n_z, rows + STAT_ROWS, LANES),
        [
            pltpu.VMEM((n_k, LANES), BF16),
            pltpu.VMEM((n_k // chunk, HEAD, chunk), BF16),
            pltpu.VMEM((steps, LANES, tile), BF16),
            pltpu.VMEM((steps, 1, tile), F32),
            pltpu.VMEM((steps, HEAD, tile), F32),
            pltpu.VMEM((steps, 1, tile), F32),
            pltpu.VMEM((2, n_k // chunk, chunk, tile), BF16),
            pltpu.VMEM((2, 8, tile), F32),
        ],
        {},
        {0, 1},
        q_all.reshape(n_q, LANES), kv_all,
        name="attend", flops=4 * 2 * n_q * n_k * 64,
    )
    parts, normed = lax.optimization_barrier((parts, normed))
    back = lax.all_to_all(parts, "z", 0, 0, tiled=True)
    ga, gb = call(
        gate_kernel,
        (shaped(rows, LANES, dtype=F32), shaped(rows, LANES, dtype=F32)),
        [],
        {},
        {0, 1, 2},
        normed, w_ga, w_gb,
        name="gates", flops=2 * rows * width * tp * 256,
    )
    gated_b = call(
        functools.partial(window_kernel, count=blocks),
        shaped(rows, LANES),
        [],
        {0, 5},
        {1, 2, 3, 4, 6},
        place, qb, kvb, before, after, sink_b, gb,
        name="windowed", flops=4 * 2 * rows * 576 * 64,
    )
    piece = shaped(n_x, rows // tp, out_a.shape[1])
    kept, sent = call(
        combine_kernel,
        (piece, piece),
        [pltpu.VMEM((tp, rows // tp, out_a.shape[1]), BF16)],
        {0},
        {1, 2, 3, 4, 5},
        place, back, ga, gated_b, out_a, out_b,
        name="combine", flops=2 * rows * 256 * 2048,
    )
    got = lax.ppermute(sent, "core", [(0, 1), (1, 0)])
    paired = (kept.astype(F32) + got.astype(F32)).astype(BF16)
    arrived = lax.all_to_all(paired, "x", 0, 0, tiled=True)
    return jnp.sum(arrived.astype(F32), axis=0).astype(BF16)


def solution(mesh):
    n_sp, n_tp = (mesh.shape["sp"], mesh.shape["tp"])
    n_z = 8
    fine = Mesh(
        np.asarray(mesh.devices).reshape(n_z, n_sp // n_z, n_tp // 2, 2), ("z", "y", "x", "core")
    )
    sp = ("z", "y")
    tp = ("x", "core")
    placed = (
        P(sp, tp), P(), P(None, tp), P(None, tp), P(None, tp), P(tp, None), P(tp, None),
        P(None, tp), P(None, tp), P(None, tp), P(tp), P(None, tp), P(None, tp), P(tp, None),
        P(tp, None),
    )
    return jax.shard_map(
        body, mesh=fine, in_specs=placed, out_specs=P((*sp, *tp), None), check_vma=False
    )
```

```python
import functools

import jax
import jax.numpy as jnp
import numpy as np
from jax import lax
from jax.experimental import pallas as pl
from jax.experimental.pallas import tpu as pltpu
from jax.sharding import Mesh, PartitionSpec as P


GRID = 64
WINDOW = 128
EPSILON = 1e-06
THETA = 10000.0
HEAD = 64
LANES = 128
BOUND = 69.0
SHIFT = 55.0
STAT_ROWS = 24
SP = ("z", "yh", "yl")
TP = ("x", "core")
F32 = jnp.float32
BF16 = jnp.bfloat16


def rotary_tables(seq, blocks):
    quarter = HEAD // 4
    freq = np.power(np.float32(THETA), -np.arange(quarter, dtype=np.float32) / np.float32(quarter))
    freq = freq.astype(np.float32)

    def table(count, which):
        angle = (np.arange(count, dtype=np.float32)[:, None] * freq).astype(np.float64)
        out = []
        for fn in (np.cos, np.sin):
            half = np.concatenate([fn(angle), fn(angle)], axis=1)
            zero = np.zeros_like(half)
            head = np.concatenate([half, zero] if which == 0 else [zero, half], axis=1)
            out.append(np.concatenate([head, head], axis=1).astype(np.float32))
        return np.stack(out)

    by_row = table(seq // GRID, 0).reshape(2, blocks, -1, LANES)
    padded = np.zeros((blocks, 16, LANES), np.float32)
    padded[:, : by_row.shape[2]] = by_row[0]
    padded[:, 8 : 8 + by_row.shape[2]] = by_row[1]
    return padded, table(GRID, 1)


def dot(a, b):
    return jnp.dot(a, b, preferred_element_type=F32)


def dot_t(a, b):
    return lax.dot_general(a, b, (((1,), (1,)), ((), ())), preferred_element_type=F32)


def silu(v):
    return v / (1.0 + jnp.exp(-v))


def rotated(n, row_s, col_ref):
    rows = n.shape[0]
    grid_rows = rows // GRID
    cos = jnp.concatenate([row_s[r : r + 1] + col_ref[0] for r in range(grid_rows)], axis=0)
    sin = jnp.concatenate([row_s[8 + r : 9 + r] + col_ref[1] for r in range(grid_rows)], axis=0)
    first = (lax.broadcasted_iota(jnp.int32, (rows, LANES), 1) % 32) < 16
    partner = jnp.where(first, -pltpu.roll(n, LANES - 16, 1), pltpu.roll(n, 16, 1))
    return n * cos + partner * sin


def key_kernel(
    place_ref, mine_ref, other_ref, gain_ref, kgain_ref, col_ref, row_ref, wka, wva,
    kv_out, h_out, h_s, narrow_s, row_s, sems,
):
    core = place_ref[0]
    copies = [pltpu.make_async_copy(row_ref.at[place_ref[1]], row_s, sems.at[2])]
    copies += [
        pltpu.make_async_copy(ref, narrow_s.at[i * HEAD : (i + 1) * HEAD], sems.at[i])
        for i, ref in enumerate((wka, wva))
    ]
    for copy in copies:
        copy.start()
    chips, rows, width = mine_ref.shape
    count = 2 * chips
    block = GRID

    def normalise(r, carry):
        at = pl.ds(pl.multiple_of(r * block, block), block)
        parts = [ref[i, at, :].astype(F32) for ref in (mine_ref, other_ref) for i in range(chips)]
        squares = functools.reduce(jnp.add, [v * v for v in parts])
        total = jnp.sum(squares, axis=1, keepdims=True)
        scale = lax.rsqrt(total / (count * width) + EPSILON)
        for n, v in enumerate(parts):
            t = 2 * (n % chips) + (core if n < chips else 1 - core)
            h_s[t, at, :] = (v * scale * gain_ref[t]).astype(BF16)
        return carry

    lax.fori_loop(0, rows // block, normalise, 0)
    normed = jnp.concatenate([h_s[t] for t in range(count)], axis=1)
    h_out[...] = normed
    for copy in copies:
        copy.wait()
    kv = dot_t(normed, narrow_s[...]).astype(BF16).astype(F32)
    low = lax.broadcasted_iota(jnp.int32, (rows, LANES), 1) < HEAD
    k_only = jnp.where(low, kv, 0.0)
    sq = jnp.sum(k_only * k_only, axis=1, keepdims=True)
    kgain = jnp.concatenate([kgain_ref[...], kgain_ref[...]], axis=1)
    ka = rotated(k_only * lax.rsqrt(sq / HEAD + EPSILON) * kgain, row_s, col_ref)
    kv_out[...] = jnp.where(low, ka, kv).astype(BF16)


def query_kernel(
    place_ref, h_ref, qgain_ref, col_ref, row_ref, wqa, wqb, wkb, wvb,
    q_out, qb_out, kvb_out, first_out, last_out, wide_s, narrow_s, row_s, sems,
):
    copies = [pltpu.make_async_copy(row_ref.at[place_ref[1]], row_s, sems.at[4])]
    copies += [
        pltpu.make_async_copy(ref, wide_s.at[i], sems.at[i]) for i, ref in enumerate((wqa, wqb))
    ]
    copies += [
        pltpu.make_async_copy(ref, narrow_s.at[i * HEAD : (i + 1) * HEAD], sems.at[2 + i])
        for i, ref in enumerate((wkb, wvb))
    ]
    for copy in copies:
        copy.start()
    for copy in copies:
        copy.wait()
    normed = h_ref[...]
    rows = normed.shape[0]
    both_q = dot(normed, jnp.concatenate([wide_s[0], wide_s[1]], axis=1))
    low = lax.broadcasted_iota(jnp.int32, (rows, LANES), 1) < HEAD
    v = both_q[:, :LANES].astype(BF16).astype(F32)
    square = v * v
    sum_low = jnp.sum(jnp.where(low, square, 0.0), axis=1, keepdims=True)
    sum_high = jnp.sum(jnp.where(low, 0.0, square), axis=1, keepdims=True)
    rs_low = lax.rsqrt(sum_low / HEAD + EPSILON)
    rs_high = lax.rsqrt(sum_high / HEAD + EPSILON)
    qgain = jnp.concatenate([qgain_ref[0:1, :], qgain_ref[1:2, :]], axis=1)
    qa = rotated(v * jnp.where(low, rs_low, rs_high) * qgain, row_s, col_ref).astype(BF16)
    for i in range(q_out.shape[0]):
        q_out[i] = qa
    qb_out[...] = both_q[:, LANES:].astype(BF16)
    kvb = dot_t(normed, narrow_s[...]).astype(BF16)
    kvb_out[...] = kvb
    first_out[...] = kvb[:WINDOW]
    last_out[...] = kvb[rows - WINDOW :]


def gate_kernel(h_ref, wa_ref, wb_ref, ga_out, gb_out):
    both = dot(h_ref[...], jnp.concatenate([wa_ref[...], wb_ref[...]], axis=1))
    gates = silu(both.astype(BF16).astype(F32))
    ga_out[...] = gates[:, :LANES]
    gb_out[...] = gates[:, LANES:]


def window_kernel(
    place_ref, q_ref, mid_ref, prev_ref, next_ref, sink_ref, gate_ref, out_ref, *, count
):
    s_index = place_ref[1]
    rows = q_ref.shape[0]
    kv = jnp.concatenate([prev_ref[...], mid_ref[...], next_ref[...]], axis=0)
    span = kv.shape[0]
    r = lax.broadcasted_iota(jnp.int32, (rows, span), 0)
    c = lax.broadcasted_iota(jnp.int32, (rows, span), 1)
    place = s_index * rows - WINDOW + c
    allowed = (c >= r) & (c - r <= 2 * WINDOW) & (place >= 0) & (place < rows * count)
    q = q_ref[...] * HEAD ** (-0.5)
    stacked = jnp.concatenate([q[:, :HEAD], q[:, HEAD:]], axis=0)
    scores = dot_t(stacked, kv[:, :HEAD])
    terms = []
    dens = []
    for h in range(2):
        s = jnp.where(allowed, scores[h * rows : (h + 1) * rows], -1e30)
        sink = sink_ref[h]
        top = jnp.maximum(jnp.max(s, axis=1, keepdims=True), sink)
        p = jnp.exp(s - top)
        dens.append(jnp.sum(p, axis=1, keepdims=True) + jnp.exp(sink - top))
        terms.append(p.astype(BF16))
    mixed = dot(jnp.concatenate(terms, axis=0), kv[:, HEAD:])
    att = jnp.concatenate([mixed[:rows] / dens[0], mixed[rows:] / dens[1]], axis=1)
    out_ref[...] = (att * gate_ref[...]).astype(BF16)


def attend_kernel(
    q_ref, kv_ref, out_ref, k_s, vt_s, qt_s, m_s, o_s, lse_s, p_s, l_s, *, tile, chunk
):
    n_q = q_ref.shape[0]
    n_k = kv_ref.shape[0]
    tiles = n_q // tile
    steps = 2 * tiles
    chunks = n_k // chunk
    kv = kv_ref[...]
    lane = lax.broadcasted_iota(jnp.int32, (n_k, LANES), 1)
    ones = jnp.where(lane < HEAD + 3, 1.0, 0.0)
    k_s[...] = jnp.where(lane < HEAD, kv.astype(F32), ones).astype(BF16)
    kv_t = kv.astype(F32).T
    k_t = kv_t[:HEAD]
    k_norm = jnp.max(jnp.sum(k_t * k_t, axis=0, keepdims=True))
    for c in range(chunks):
        vt_s[c] = kv_t[HEAD:, c * chunk : (c + 1) * chunk].astype(BF16)
    top = jnp.float32(0.0)
    for i in range(tiles):
        q_t = q_ref[i * tile : (i + 1) * tile, :].astype(F32).T
        for h in range(2):
            part = q_t[h * HEAD : (h + 1) * HEAD] * HEAD ** (-0.5)
            bound = jnp.sqrt(jnp.sum(part * part, axis=0, keepdims=True) * k_norm) * 1.0001
            top = jnp.maximum(top, jnp.max(bound))
            m_s[2 * i + h] = bound - SHIFT
            qt_s[2 * i + h, :HEAD] = part.astype(BF16)
            qt_s[2 * i + h, HEAD:] = jnp.zeros((LANES - HEAD, tile), BF16)

    @pl.when(top > BOUND)
    def _():
        def row_max(t, carry):
            def one(c, m):
                s = dot(k_s[pl.ds(pl.multiple_of(c * chunk, chunk), chunk), :], qt_s[t])
                return jnp.maximum(m, jnp.max(s, axis=0, keepdims=True))

            m_s[t] = lax.fori_loop(0, chunks, one, jnp.full((1, tile), -1e30, F32))
            return carry

        lax.fori_loop(0, steps, row_max, 0)

    row = lax.broadcasted_iota(jnp.int32, (16, tile), 0)
    for t in range(steps):
        neg = -m_s[t]
        hi = neg.astype(BF16).astype(F32)
        mid = (neg - hi).astype(BF16).astype(F32)
        lo = neg - hi - mid
        parts = jnp.where(row == 0, hi, jnp.where(row == 1, mid, jnp.where(row == 2, lo, 0.0)))
        qt_s[t, HEAD : HEAD + 16] = parts.astype(BF16)

    def both(ahead, ahead_slot, now, now_slot):
        if ahead is not None:
            q_here = qt_s[ahead]
            sums = jnp.zeros((8, tile), F32)
        acc = jnp.zeros((HEAD, tile), F32)
        for c in range(chunks):
            if ahead is not None:
                e = jnp.exp(dot(k_s[c * chunk : (c + 1) * chunk, :], q_here))
                sums = sums + jnp.sum(e.reshape(chunk // 8, 8, tile), axis=0)
                p_s[ahead_slot, c] = e.astype(BF16)
            if now is not None:
                acc = acc + dot(vt_s[c], p_s[now_slot, c])
        if now is not None:
            total = jnp.sum(l_s[now_slot], axis=0, keepdims=True)
            lse_s[now] = m_s[now] + jnp.log(total)
            o_s[now] = acc / total
        if ahead is not None:
            l_s[ahead_slot] = sums

    both(0, 0, None, None)

    def pair(n, carry):
        both(2 * n + 1, 1, 2 * n, 0)
        both(2 * n + 2, 0, 2 * n + 1, 1)
        return carry

    lax.fori_loop(0, (steps - 2) // 2, pair, 0)
    both(steps - 1, 1, steps - 2, 0)
    both(None, None, steps - 1, 1)

    lse = jnp.concatenate(
        [jnp.concatenate([lse_s[2 * i], lse_s[2 * i + 1]], axis=0) for i in range(tiles)], axis=1
    )
    hi = lse.astype(BF16).astype(F32)
    mid = (lse - hi).astype(BF16).astype(F32)
    lo = lse - hi - mid
    stats = jnp.concatenate([hi, mid, lo, jnp.zeros_like(hi)], axis=0)
    stats = jnp.concatenate([stats, jnp.zeros((8, LANES), F32)], axis=1)
    blocks = out_ref.shape[0]
    rows = n_q // blocks
    flat = jnp.concatenate(
        [
            jnp.concatenate([o_s[2 * i], o_s[2 * i + 1]], axis=0).T.astype(BF16)
            for i in range(tiles)
        ],
        axis=0,
    )
    for b in range(blocks):
        out_ref[b, :rows] = flat[b * rows : (b + 1) * rows]
        for k in range(STAT_ROWS // 8):
            at = b * rows + k * LANES
            out_ref[b, rows + 8 * k : rows + 8 * k + 8] = stats[:, at : at + LANES].astype(BF16)


def combine_kernel(
    place_ref, part_ref, ga_ref, gated_b_ref, wa_ref, wb_ref, kept_ref, sent_ref, out_s
):
    blocks, padded, _ = part_ref.shape
    rows = padded - STAT_ROWS
    lses = []
    for s in range(blocks):
        pieces = [
            part_ref[s, rows + 8 * k : rows + 8 * k + 8].astype(F32) for k in range(STAT_ROWS // 8)
        ]
        x = jnp.concatenate(pieces, axis=1)
        lses.append(x[0:2] + x[2:4] + x[4:6])
    top = functools.reduce(jnp.maximum, lses)
    weights = [jnp.exp(v - top) for v in lses]
    den = functools.reduce(jnp.add, weights)
    stacked = jnp.concatenate([v / den for v in weights], axis=0)
    cols = jnp.concatenate(
        [stacked, jnp.zeros((LANES - 2 * blocks, stacked.shape[1]), F32)], axis=0
    ).T
    low = lax.broadcasted_iota(jnp.int32, (rows, LANES), 1) < HEAD
    acc = jnp.zeros((rows, LANES), F32)
    for s in range(blocks):
        w = jnp.where(low, cols[:rows, 2 * s : 2 * s + 1], cols[:rows, 2 * s + 1 : 2 * s + 2])
        acc = acc + w * part_ref[s, :rows].astype(F32)
    gated_a = (acc * ga_ref[...]).astype(BF16)
    gated = jnp.concatenate([gated_a, gated_b_ref[...]], axis=1)
    w = jnp.concatenate([wa_ref[...], wb_ref[...]], axis=0)
    result = dot(gated, w).astype(BF16)
    core = place_ref[0]
    chips, piece, _ = kept_ref.shape
    for t in range(2 * chips):
        out_s[t] = result[t * piece : (t + 1) * piece]
    for i in range(chips):
        kept_ref[i] = out_s[2 * i + core]
        sent_ref[i] = out_s[2 * i + 1 - core]


def call(kernel, outs, scratch, smem, near, *args, flops=0, far=()):
    args = [
        pltpu.with_memory_space_constraint(a, pltpu.VMEM) if i in near else a
        for i, a in enumerate(args)
    ]
    specs = [
        pl.BlockSpec(
            memory_space=pltpu.SMEM if i in smem else pl.ANY if i in far else pltpu.VMEM
        )
        for i in range(len(args))
    ]
    return pl.pallas_call(
        kernel,
        out_shape=outs,
        in_specs=specs,
        out_specs=(
            tuple(pl.BlockSpec(memory_space=pltpu.VMEM) for _ in outs)
            if isinstance(outs, tuple)
            else pl.BlockSpec(memory_space=pltpu.VMEM)
        ),
        scratch_shapes=scratch,
        compiler_params=pltpu.CompilerParams(vmem_limit_bytes=56 * 2**20),
        cost_estimate=pl.CostEstimate(flops=flops, bytes_accessed=2**20, transcendentals=0),
    )(*args)


def shaped(*shape, dtype=BF16):
    return pltpu.VMEM(shape, dtype)


def body(
    tokens, norm_gain, w_qa, w_ka, w_va, qgain_a, kgain_a, w_qb, w_kb, w_vb, sink_b, w_ga, w_gb,
    out_a, out_b,
):
    rows, width = tokens.shape
    n_z, n_x = (lax.axis_size(a) for a in ("z", "x"))
    n_y = lax.axis_size("yh") * lax.axis_size("yl")
    blocks = n_z * n_y
    tp = 2 * n_x
    s_index = lax.axis_index(SP)
    core = lax.axis_index("core")
    place = jnp.stack([core, s_index]).astype(jnp.int32)
    row_table, col_table = rotary_tables(blocks * rows, blocks)

    mine = lax.all_gather(tokens, "x", axis=0)
    other = lax.ppermute(mine, "core", [(0, 1), (1, 0)])
    col_table = jnp.asarray(col_table)
    row_table = jnp.asarray(row_table)
    kv, normed = call(
        key_kernel,
        (shaped(rows, LANES), shaped(rows, tp * width)),
        [
            pltpu.VMEM((tp, rows, width), BF16),
            pltpu.VMEM((2 * HEAD, tp * width), BF16),
            pltpu.VMEM((16, LANES), F32),
            pltpu.SemaphoreType.DMA((3,)),
        ],
        {0},
        {1, 2},
        place, mine, other, norm_gain.reshape(tp, 1, width), kgain_a, col_table, row_table,
        w_ka.T, w_va.T,
        flops=2 * rows * width * tp * 128, far={6, 7, 8},
    )
    kv_far = lax.ppermute(kv, "yh", [(0, 1), (1, 0)])
    q8, qb, kvb, kvb_first, kvb_last = call(
        query_kernel,
        (
            shaped(n_z, rows, LANES), shaped(rows, LANES), shaped(rows, LANES),
            shaped(WINDOW, LANES), shaped(WINDOW, LANES),
        ),
        [
            pltpu.VMEM((2, tp * width, LANES), BF16),
            pltpu.VMEM((2 * HEAD, tp * width), BF16),
            pltpu.VMEM((16, LANES), F32),
            pltpu.SemaphoreType.DMA((5,)),
        ],
        {0},
        {1},
        place, normed, qgain_a, col_table, row_table, w_qa, w_qb, w_kb.T, w_vb.T,
        flops=2 * rows * width * tp * 384, far={4, 5, 6, 7, 8},
    )
    q_all = lax.all_to_all(q8, "z", 0, 0, tiled=True)
    kv_pair = jnp.concatenate([kv, kv_far], axis=0)
    kv_all = lax.all_gather(kv_pair, "yl", axis=0, tiled=True)
    up = [(i, i + 1) for i in range(blocks - 1)]
    down = [(i + 1, i) for i in range(blocks - 1)]
    before = lax.ppermute(kvb_last, SP, up)
    after = lax.ppermute(kvb_first, SP, down)
    n_q = n_z * rows
    n_k = n_y * rows
    tile = 512
    chunk = 256
    steps = 2 * n_q // tile
    parts = call(
        functools.partial(attend_kernel, tile=tile, chunk=chunk),
        shaped(n_z, rows + STAT_ROWS, LANES),
        [
            pltpu.VMEM((n_k, LANES), BF16),
            pltpu.VMEM((n_k // chunk, HEAD, chunk), BF16),
            pltpu.VMEM((steps, LANES, tile), BF16),
            pltpu.VMEM((steps, 1, tile), F32),
            pltpu.VMEM((steps, HEAD, tile), F32),
            pltpu.VMEM((steps, 1, tile), F32),
            pltpu.VMEM((2, n_k // chunk, chunk, tile), BF16),
            pltpu.VMEM((2, 8, tile), F32),
        ],
        {},
        {0, 1},
        q_all.reshape(n_q, LANES), kv_all,
        flops=4 * 2 * n_q * n_k * 64,
    )
    parts, normed = lax.optimization_barrier((parts, normed))
    back = lax.all_to_all(parts, "z", 0, 0, tiled=True)
    ga, gb = call(
        gate_kernel,
        (shaped(rows, LANES, dtype=F32), shaped(rows, LANES, dtype=F32)),
        [],
        {},
        {0, 1, 2},
        normed, w_ga, w_gb,
        flops=2 * rows * width * tp * 256,
    )
    gated_b = call(
        functools.partial(window_kernel, count=blocks),
        shaped(rows, LANES),
        [],
        {0, 5},
        {1, 2, 3, 4, 6},
        place, qb, kvb, before, after, sink_b, gb,
        flops=4 * 2 * rows * 576 * 64,
    )
    piece = shaped(n_x, rows // tp, out_a.shape[1])
    kept, sent = call(
        combine_kernel,
        (piece, piece),
        [pltpu.VMEM((tp, rows // tp, out_a.shape[1]), BF16)],
        {0},
        {1, 2, 3, 4, 5},
        place, back, ga, gated_b, out_a, out_b,
        flops=2 * rows * 256 * 2048,
    )
    got = lax.ppermute(sent, "core", [(0, 1), (1, 0)])
    paired = (kept.astype(F32) + got.astype(F32)).astype(BF16)
    arrived = lax.all_to_all(paired, "x", 0, 0, tiled=True)
    return jnp.sum(arrived.astype(F32), axis=0).astype(BF16)


def solution(mesh):
    n_tp = mesh.shape["tp"]
    fine = Mesh(np.asarray(mesh.devices).reshape(8, 2, 4, n_tp // 2, 2), (*SP, *TP))
    sp = SP
    tp = TP
    placed = (
        P(sp, tp), P(), P(None, tp), P(None, tp), P(None, tp), P(tp, None), P(tp, None),
        P(None, tp), P(None, tp), P(None, tp), P(tp), P(None, tp), P(None, tp), P(tp, None),
        P(tp, None),
    )
    return jax.shard_map(
        body, mesh=fine, in_specs=placed, out_specs=P((*sp, *tp), None), check_vma=False
    )
```

```python
import functools

import jax
import jax.numpy as jnp
import numpy as np
from jax import lax
from jax.experimental import pallas as pl
from jax.experimental.pallas import tpu as pltpu
from jax.sharding import Mesh, PartitionSpec as P

GRID = 64
WINDOW = 128
EPSILON = 1e-06
THETA = 10000.0
HEAD = 64
LANES = 128
BOUND = 69.0
SHIFT = 55.0
STAT_ROWS = 24
F32 = jnp.float32
BF16 = jnp.bfloat16


def rotary_tables(seq, blocks):
    quarter = HEAD // 4
    freq = np.power(np.float32(THETA), -np.arange(quarter, dtype=np.float32) / np.float32(quarter))
    freq = freq.astype(np.float32)

    def table(count, which):
        angle = (np.arange(count, dtype=np.float32)[:, None] * freq).astype(np.float64)
        out = []
        for fn in (np.cos, np.sin):
            half = np.concatenate([fn(angle), fn(angle)], axis=1)
            zero = np.zeros_like(half)
            head = np.concatenate([half, zero] if which == 0 else [zero, half], axis=1)
            out.append(np.concatenate([head, head], axis=1).astype(np.float32))
        return np.stack(out)

    by_row = table(seq // GRID, 0).reshape(2, blocks, -1, LANES)
    padded = np.zeros((blocks, 16, LANES), np.float32)
    padded[:, : by_row.shape[2]] = by_row[0]
    padded[:, 8 : 8 + by_row.shape[2]] = by_row[1]
    return padded, table(GRID, 1)


def dot(a, b):
    return jnp.dot(a, b, preferred_element_type=F32)


def dot_t(a, b):
    return lax.dot_general(a, b, (((1,), (1,)), ((), ())), preferred_element_type=F32)


def silu(v):
    return v / (1.0 + jnp.exp(-v))


def project_kernel(
    place_ref, mine_ref, other_ref, gain_ref, qgain_ref, kgain_ref, col_ref, row_ref,
    wqa, wka, wva, wqb, wkb, wvb,
    q_out, kv_out, qb_out, kvb_out, first_out, last_out, h_out,
    h_s, wide_s, narrow_s, row_s, sems,
):
    core = place_ref[0]
    wide = [wqa, wqb]
    narrow = [wka, wva, wkb, wvb]
    copies = [pltpu.make_async_copy(row_ref.at[place_ref[1]], row_s, sems.at[6])]
    copies += [
        pltpu.make_async_copy(ref, narrow_s.at[i * HEAD : (i + 1) * HEAD], sems.at[i])
        for i, ref in enumerate(narrow)
    ]
    copies += [
        pltpu.make_async_copy(ref, wide_s.at[i], sems.at[4 + i]) for i, ref in enumerate(wide)
    ]
    for copy in copies:
        copy.start()
    chips, rows, width = mine_ref.shape
    count = 2 * chips
    block = GRID

    def normalise(r, carry):
        at = pl.ds(pl.multiple_of(r * block, block), block)
        parts = [ref[i, at, :].astype(F32) for ref in (mine_ref, other_ref) for i in range(chips)]
        squares = functools.reduce(jnp.add, [v * v for v in parts])
        total = jnp.sum(squares, axis=1, keepdims=True)
        scale = lax.rsqrt(total / (count * width) + EPSILON)
        for n, v in enumerate(parts):
            t = 2 * (n % chips) + (core if n < chips else 1 - core)
            h_s[t, at, :] = (v * scale * gain_ref[t]).astype(BF16)
        return carry

    lax.fori_loop(0, rows // block, normalise, 0)
    normed = jnp.concatenate([h_s[t] for t in range(count)], axis=1)
    h_out[...] = normed
    for copy in copies:
        copy.wait()
    both_kv = dot_t(normed, narrow_s[...])
    both_q = dot(normed, jnp.concatenate([wide_s[0], wide_s[1]], axis=1))
    qb_out[...] = both_q[:, LANES:].astype(BF16)
    kvb = both_kv[:, LANES:].astype(BF16)
    kvb_out[...] = kvb
    first_out[...] = kvb[:WINDOW]
    last_out[...] = kvb[rows - WINDOW :]
    grid_rows = rows // GRID
    cos = jnp.concatenate([row_s[r : r + 1] + col_ref[0] for r in range(grid_rows)], axis=0)
    sin = jnp.concatenate([row_s[8 + r : 9 + r] + col_ref[1] for r in range(grid_rows)], axis=0)
    lane = lax.broadcasted_iota(jnp.int32, (rows, LANES), 1)
    first = (lane % 32) < 16
    low = lane < HEAD

    def turned(n):
        partner = jnp.where(first, -pltpu.roll(n, LANES - 16, 1), pltpu.roll(n, 16, 1))
        return n * cos + partner * sin

    v = both_q[:, :LANES].astype(BF16).astype(F32)
    square = v * v
    sum_low = jnp.sum(jnp.where(low, square, 0.0), axis=1, keepdims=True)
    sum_high = jnp.sum(jnp.where(low, 0.0, square), axis=1, keepdims=True)
    rs_low = lax.rsqrt(sum_low / HEAD + EPSILON)
    rs_high = lax.rsqrt(sum_high / HEAD + EPSILON)
    qgain = jnp.concatenate([qgain_ref[0:1, :], qgain_ref[1:2, :]], axis=1)
    q_out[...] = turned(v * jnp.where(low, rs_low, rs_high) * qgain).astype(BF16)
    kv = both_kv[:, :LANES].astype(BF16).astype(F32)
    k_only = jnp.where(low, kv, 0.0)
    sq = jnp.sum(k_only * k_only, axis=1, keepdims=True)
    kgain = jnp.concatenate([kgain_ref[...], kgain_ref[...]], axis=1)
    ka = turned(k_only * lax.rsqrt(sq / HEAD + EPSILON) * kgain)
    both = jnp.where(low, ka, kv).astype(BF16)
    for i in range(kv_out.shape[0]):
        kv_out[i] = both


def gate_kernel(h_ref, wa_ref, wb_ref, ga_out, gb_out):
    both = dot(h_ref[...], jnp.concatenate([wa_ref[...], wb_ref[...]], axis=1))
    gates = silu(both.astype(BF16).astype(F32))
    ga_out[...] = gates[:, :LANES]
    gb_out[...] = gates[:, LANES:]


def window_kernel(
    place_ref, q_ref, mid_ref, prev_ref, next_ref, sink_ref, gate_ref, out_ref, *, count
):
    s_index = place_ref[1]
    rows = q_ref.shape[0]
    kv = jnp.concatenate([prev_ref[...], mid_ref[...], next_ref[...]], axis=0)
    span = kv.shape[0]
    r = lax.broadcasted_iota(jnp.int32, (rows, span), 0)
    c = lax.broadcasted_iota(jnp.int32, (rows, span), 1)
    place = s_index * rows - WINDOW + c
    allowed = (c >= r) & (c - r <= 2 * WINDOW) & (place >= 0) & (place < rows * count)
    q = q_ref[...] * HEAD ** (-0.5)
    stacked = jnp.concatenate([q[:, :HEAD], q[:, HEAD:]], axis=0)
    scores = dot_t(stacked, kv[:, :HEAD])
    terms = []
    dens = []
    for h in range(2):
        s = jnp.where(allowed, scores[h * rows : (h + 1) * rows], -1e30)
        sink = sink_ref[h]
        top = jnp.maximum(jnp.max(s, axis=1, keepdims=True), sink)
        p = jnp.exp(s - top)
        dens.append(jnp.sum(p, axis=1, keepdims=True) + jnp.exp(sink - top))
        terms.append(p.astype(BF16))
    mixed = dot(jnp.concatenate(terms, axis=0), kv[:, HEAD:])
    att = jnp.concatenate([mixed[:rows] / dens[0], mixed[rows:] / dens[1]], axis=1)
    out_ref[...] = (att * gate_ref[...]).astype(BF16)


def attend_kernel(
    q_ref, kv_ref, out_ref, k_s, vt_s, qt_s, m_s, o_s, lse_s, p_s, l_s, *, tile, chunk
):
    n_q = q_ref.shape[0]
    n_k = kv_ref.shape[0]
    tiles = n_q // tile
    steps = 2 * tiles
    chunks = n_k // chunk
    kv = kv_ref[...]
    lane = lax.broadcasted_iota(jnp.int32, (n_k, LANES), 1)
    ones = jnp.where(lane < HEAD + 3, 1.0, 0.0)
    k_s[...] = jnp.where(lane < HEAD, kv.astype(F32), ones).astype(BF16)
    kv_t = kv.astype(F32).T
    k_t = kv_t[:HEAD]
    k_norm = jnp.max(jnp.sum(k_t * k_t, axis=0, keepdims=True))
    for c in range(chunks):
        vt_s[c] = kv_t[HEAD:, c * chunk : (c + 1) * chunk].astype(BF16)
    top = jnp.float32(0.0)
    for i in range(tiles):
        q_t = q_ref[i * tile : (i + 1) * tile, :].astype(F32).T
        for h in range(2):
            part = q_t[h * HEAD : (h + 1) * HEAD] * HEAD ** (-0.5)
            bound = jnp.sqrt(jnp.sum(part * part, axis=0, keepdims=True) * k_norm) * 1.0001
            top = jnp.maximum(top, jnp.max(bound))
            m_s[2 * i + h] = bound - SHIFT
            qt_s[2 * i + h, :HEAD] = part.astype(BF16)
            qt_s[2 * i + h, HEAD:] = jnp.zeros((LANES - HEAD, tile), BF16)

    @pl.when(top > BOUND)
    def _():
        def row_max(t, carry):
            def one(c, m):
                s = dot(k_s[pl.ds(pl.multiple_of(c * chunk, chunk), chunk), :], qt_s[t])
                return jnp.maximum(m, jnp.max(s, axis=0, keepdims=True))

            m_s[t] = lax.fori_loop(0, chunks, one, jnp.full((1, tile), -1e30, F32))
            return carry

        lax.fori_loop(0, steps, row_max, 0)

    row = lax.broadcasted_iota(jnp.int32, (16, tile), 0)
    for t in range(steps):
        neg = -m_s[t]
        hi = neg.astype(BF16).astype(F32)
        mid = (neg - hi).astype(BF16).astype(F32)
        lo = neg - hi - mid
        parts = jnp.where(row == 0, hi, jnp.where(row == 1, mid, jnp.where(row == 2, lo, 0.0)))
        qt_s[t, HEAD : HEAD + 16] = parts.astype(BF16)

    def both(ahead, ahead_slot, now, now_slot):
        if ahead is not None:
            q_here = qt_s[ahead]
            sums = jnp.zeros((8, tile), F32)
        acc = jnp.zeros((HEAD, tile), F32)
        for c in range(chunks):
            if ahead is not None:
                e = jnp.exp(dot(k_s[c * chunk : (c + 1) * chunk, :], q_here))
                sums = sums + jnp.sum(e.reshape(chunk // 8, 8, tile), axis=0)
                p_s[ahead_slot, c] = e.astype(BF16)
            if now is not None:
                acc = acc + dot(vt_s[c], p_s[now_slot, c])
        if now is not None:
            total = jnp.sum(l_s[now_slot], axis=0, keepdims=True)
            lse_s[now] = m_s[now] + jnp.log(total)
            o_s[now] = acc / total
        if ahead is not None:
            l_s[ahead_slot] = sums

    both(0, 0, None, None)

    def pair(n, carry):
        both(2 * n + 1, 1, 2 * n, 0)
        both(2 * n + 2, 0, 2 * n + 1, 1)
        return carry

    lax.fori_loop(0, (steps - 2) // 2, pair, 0)
    both(steps - 1, 1, steps - 2, 0)
    both(None, None, steps - 1, 1)

    lse = jnp.concatenate(
        [jnp.concatenate([lse_s[2 * i], lse_s[2 * i + 1]], axis=0) for i in range(tiles)], axis=1
    )
    hi = lse.astype(BF16).astype(F32)
    mid = (lse - hi).astype(BF16).astype(F32)
    lo = lse - hi - mid
    stats = jnp.concatenate([hi, mid, lo, jnp.zeros_like(hi)], axis=0)
    stats = jnp.concatenate([stats, jnp.zeros((8, LANES), F32)], axis=1)
    blocks = out_ref.shape[0]
    rows = n_q // blocks
    flat = jnp.concatenate(
        [
            jnp.concatenate([o_s[2 * i], o_s[2 * i + 1]], axis=0).T.astype(BF16)
            for i in range(tiles)
        ],
        axis=0,
    )
    for b in range(blocks):
        out_ref[b, :rows] = flat[b * rows : (b + 1) * rows]
        for k in range(STAT_ROWS // 8):
            at = b * rows + k * LANES
            out_ref[b, rows + 8 * k : rows + 8 * k + 8] = stats[:, at : at + LANES].astype(BF16)


def combine_kernel(
    place_ref, part_ref, ga_ref, gated_b_ref, wa_ref, wb_ref, kept_ref, sent_ref, out_s
):
    blocks, padded, _ = part_ref.shape
    rows = padded - STAT_ROWS
    lses = []
    for s in range(blocks):
        pieces = [
            part_ref[s, rows + 8 * k : rows + 8 * k + 8].astype(F32) for k in range(STAT_ROWS // 8)
        ]
        x = jnp.concatenate(pieces, axis=1)
        lses.append(x[0:2] + x[2:4] + x[4:6])
    top = functools.reduce(jnp.maximum, lses)
    weights = [jnp.exp(v - top) for v in lses]
    den = functools.reduce(jnp.add, weights)
    stacked = jnp.concatenate([v / den for v in weights], axis=0)
    cols = jnp.concatenate(
        [stacked, jnp.zeros((LANES - 2 * blocks, stacked.shape[1]), F32)], axis=0
    ).T
    low = lax.broadcasted_iota(jnp.int32, (rows, LANES), 1) < HEAD
    acc = jnp.zeros((rows, LANES), F32)
    for s in range(blocks):
        w = jnp.where(low, cols[:rows, 2 * s : 2 * s + 1], cols[:rows, 2 * s + 1 : 2 * s + 2])
        acc = acc + w * part_ref[s, :rows].astype(F32)
    gated_a = (acc * ga_ref[...]).astype(BF16)
    gated = jnp.concatenate([gated_a, gated_b_ref[...]], axis=1)
    w = jnp.concatenate([wa_ref[...], wb_ref[...]], axis=0)
    result = dot(gated, w).astype(BF16)
    core = place_ref[0]
    chips, piece, _ = kept_ref.shape
    for t in range(2 * chips):
        out_s[t] = result[t * piece : (t + 1) * piece]
    for i in range(chips):
        kept_ref[i] = out_s[2 * i + core]
        sent_ref[i] = out_s[2 * i + 1 - core]


def call(kernel, outs, scratch, smem, near, *args, name, flops=0, far=()):
    args = [
        pltpu.with_memory_space_constraint(a, pltpu.VMEM) if i in near else a
        for i, a in enumerate(args)
    ]
    specs = [
        pl.BlockSpec(
            memory_space=pltpu.SMEM if i in smem else pl.ANY if i in far else pltpu.VMEM
        )
        for i in range(len(args))
    ]
    return pl.pallas_call(
        kernel,
        out_shape=outs,
        in_specs=specs,
        out_specs=(
            tuple(pl.BlockSpec(memory_space=pltpu.VMEM) for _ in outs)
            if isinstance(outs, tuple)
            else pl.BlockSpec(memory_space=pltpu.VMEM)
        ),
        scratch_shapes=scratch,
        compiler_params=pltpu.CompilerParams(vmem_limit_bytes=56 * 2**20),
        cost_estimate=pl.CostEstimate(flops=flops, bytes_accessed=2**20, transcendentals=0),
        name=name,
    )(*args)


def shaped(*shape, dtype=BF16):
    return pltpu.VMEM(shape, dtype)


def body(
    tokens, norm_gain, w_qa, w_ka, w_va, qgain_a, kgain_a, w_qb, w_kb, w_vb, sink_b, w_ga, w_gb,
    out_a, out_b,
):
    rows, width = tokens.shape
    n_z, n_y, n_x = (lax.axis_size(a) for a in ("z", "y", "x"))
    blocks = n_z * n_y
    tp = 2 * n_x
    s_index = lax.axis_index("z") * n_y + lax.axis_index("y")
    core = lax.axis_index("core")
    place = jnp.stack([core, s_index]).astype(jnp.int32)
    row_table, col_table = rotary_tables(blocks * rows, blocks)

    mine = lax.all_gather(tokens, "x", axis=0)
    other = lax.ppermute(mine, "core", [(0, 1), (1, 0)])
    q, kv8, qb, kvb, kvb_first, kvb_last, normed = call(
        project_kernel,
        (
            shaped(rows, LANES), shaped(n_z, rows, LANES),
            shaped(rows, LANES), shaped(rows, LANES),
            shaped(WINDOW, LANES), shaped(WINDOW, LANES),
            shaped(rows, tp * width),
        ),
        [
            pltpu.VMEM((tp, rows, width), BF16),
            pltpu.VMEM((2, tp * width, LANES), BF16),
            pltpu.VMEM((4 * HEAD, tp * width), BF16),
            pltpu.VMEM((16, LANES), F32),
            pltpu.SemaphoreType.DMA((7,)),
        ],
        {0},
        {1, 2},
        place, mine, other, norm_gain.reshape(tp, 1, width), qgain_a, kgain_a,
        jnp.asarray(col_table), jnp.asarray(row_table),
        w_qa, w_ka.T, w_va.T, w_qb, w_kb.T, w_vb.T,
        name="project", flops=2 * rows * width * tp * 512, far=set(range(7, 14)),
    )
    kv_all = lax.all_to_all(kv8, "z", 0, 0, tiled=True)
    q_all = lax.all_gather(q, "y", axis=0, tiled=True)
    up = [(i, i + 1) for i in range(blocks - 1)]
    down = [(i + 1, i) for i in range(blocks - 1)]
    before = lax.ppermute(kvb_last, ("z", "y"), up)
    after = lax.ppermute(kvb_first, ("z", "y"), down)
    n_q = n_y * rows
    n_k = n_z * rows
    tile = 512
    chunk = 256
    steps = 2 * n_q // tile
    parts = call(
        functools.partial(attend_kernel, tile=tile, chunk=chunk),
        shaped(n_y, rows + STAT_ROWS, LANES),
        [
            pltpu.VMEM((n_k, LANES), BF16),
            pltpu.VMEM((n_k // chunk, HEAD, chunk), BF16),
            pltpu.VMEM((steps, LANES, tile), BF16),
            pltpu.VMEM((steps, 1, tile), F32),
            pltpu.VMEM((steps, HEAD, tile), F32),
            pltpu.VMEM((steps, 1, tile), F32),
            pltpu.VMEM((2, n_k // chunk, chunk, tile), BF16),
            pltpu.VMEM((2, 8, tile), F32),
        ],
        {},
        {0, 1},
        q_all, kv_all.reshape(n_k, LANES),
        name="attend", flops=4 * 2 * n_q * n_k * 64,
    )
    parts, normed = lax.optimization_barrier((parts, normed))
    back = lax.all_to_all(parts, "y", 0, 0, tiled=True)
    ga, gb = call(
        gate_kernel,
        (shaped(rows, LANES, dtype=F32), shaped(rows, LANES, dtype=F32)),
        [],
        {},
        {0, 1, 2},
        normed, w_ga, w_gb,
        name="gates", flops=2 * rows * width * tp * 256,
    )
    gated_b = call(
        functools.partial(window_kernel, count=blocks),
        shaped(rows, LANES),
        [],
        {0, 5},
        {1, 2, 3, 4, 6},
        place, qb, kvb, before, after, sink_b, gb,
        name="windowed", flops=4 * 2 * rows * 576 * 64,
    )
    piece = shaped(n_x, rows // tp, out_a.shape[1])
    kept, sent = call(
        combine_kernel,
        (piece, piece),
        [pltpu.VMEM((tp, rows // tp, out_a.shape[1]), BF16)],
        {0},
        {1, 2, 3, 4, 5},
        place, back, ga, gated_b, out_a, out_b,
        name="combine", flops=2 * rows * 256 * 2048,
    )
    got = lax.ppermute(sent, "core", [(0, 1), (1, 0)])
    paired = (kept.astype(F32) + got.astype(F32)).astype(BF16)
    arrived = lax.all_to_all(paired, "x", 0, 0, tiled=True)
    return jnp.sum(arrived.astype(F32), axis=0).astype(BF16)


def solution(mesh):
    n_sp, n_tp = (mesh.shape["sp"], mesh.shape["tp"])
    n_z = 8
    fine = Mesh(
        np.asarray(mesh.devices).reshape(n_z, n_sp // n_z, n_tp // 2, 2), ("z", "y", "x", "core")
    )
    sp = ("z", "y")
    tp = ("x", "core")
    placed = (
        P(sp, tp), P(), P(None, tp), P(None, tp), P(None, tp), P(tp, None), P(tp, None),
        P(None, tp), P(None, tp), P(None, tp), P(tp), P(None, tp), P(None, tp), P(tp, None),
        P(tp, None),
    )
    return jax.shard_map(
        body, mesh=fine, in_specs=placed, out_specs=P((*sp, *tp), None), check_vma=False
    )
```
